32 devices in a mesh: sp: 16 (over z, y, x), tp: 2 (over core).
Axes of the slice: x: 2, y: 2, z: 4, core: 2. Of those that a mesh axis runs over, the one named last changes fastest.
Arguments:
- queries: bfloat16 [8192, 1024], P('sp', 'tp'), may hold values from -8 to 8
- key_rows: bfloat16 [8192, 512], P('sp', 'tp'), may hold values from -8 to 8
- values: bfloat16 [8192, 512], P('sp', 'tp'), may hold values from -16 to 16
- doc_ids: int32 [8192], P('sp'), may hold values from 0 to 7, never falling along the last dimension, each value on 1 to 2048 neighbouring positions
- sink_logits: float32 [16], P('tp'), may hold values from 2.5 to 6
- residual: bfloat16 [8192, 2048], P('sp'), may hold values from -6 to 6
- out_weight: bfloat16 [1024, 2048], P('tp'), may hold values from -0.1875 to 0.1875
- norm_gain: float32 [2048], replicated, may hold values from 0.1 to 1.9
- w_gate: bfloat16 [2048, 5632], P('sp', 'tp'), may hold values from -0.125 to 0.125
- w_up: bfloat16 [2048, 5632], P('sp', 'tp'), may hold values from -0.125 to 0.125
- w_down: bfloat16 [5632, 2048], P('tp', 'sp'), may hold values from -0.078125 to 0.078125
Outputs:
- layer_out: bfloat16 [8192, 2048], P('sp')
The draws below stay inside these ranges and needn't reach their ends.
Inputs may be any that keep to these rules, and one draw needn't show every extreme that they name: `doc_ids`: document numbers never fall along the positions; each document has 1 to 2048 positions.
All inputs are finite; a program needn't handle non-finite values.
Results may differ from the reference program's by a relative error of at most 0.014.
Values may be sent and summed in bfloat16 or wider, within the bound.
A program may use at most 128 MiB of HBM per device.

```python
import math
import jax
import jax.numpy as jnp
import numpy as np
from jax import lax

D = 2048
HEADS = 16
KV_HEADS = 8
HD = 64
FF = 5632
WINDOW = 128
TOKENS = 8192
DOCS = 8
DOC_MOST = 2048
N_TP = 2


def drawn_pair(key):
    query_key = jax.random.fold_in(key, 101)
    row_key = jax.random.fold_in(key, 102)
    queries = jnp.clip(jax.random.normal(query_key, (TOKENS, HEADS * HD), jnp.float32), -6.0, 6.0)
    key_rows = jnp.clip(jax.random.normal(row_key, (TOKENS, KV_HEADS * HD), jnp.float32), -6.0, 6.0)
    return (queries, key_rows)


def draw_queries(key, part):
    return drawn_pair(key)[0].astype(jnp.bfloat16)


def draw_key_rows(key, part):
    return drawn_pair(key)[1].astype(jnp.bfloat16)


def steps_of(stream_key, dims, split, low, high):
    loudness, own = 1.0, jax.random.fold_in(stream_key, 6)
    for position, shards_of in split:
        steps = jnp.exp(jax.random.uniform(jax.random.fold_in(own, position), (shards_of,), jnp.float32, low / len(split), high / len(split)))
        loudness = loudness * jnp.repeat(steps, dims[position] // shards_of).reshape([-1 if axis == position else 1 for axis in range(len(dims))])
    return loudness


def split_up(number_of, total, most, skew):
    loads = [(1 << 20) // math.isqrt(grade ** skew) + 1 for grade in range(2, number_of + 1)]
    rest, given = total - most - (number_of - 1), [1] * (number_of - 1)
    while rest > 0:
        candidates = [i for i in range(number_of - 1) if given[i] < most]
        pool, remaining = sum([loads[i] for i in candidates]), rest
        for i in candidates:
            more = min(most - given[i], max(1, remaining * loads[i] // pool), rest)
            given[i] = given[i] + more
            rest = rest - more
    return np.array([most] + given)


def uneven_parts(stream_key, amount, total, reach, slope):
    if amount == 2:
        one = jax.random.randint(stream_key, (), max(1, total - reach), min(reach, total - 1) + 1)
        return jnp.stack([one, total - one])
    lengths = jnp.asarray(split_up(amount, total, reach, slope), jnp.int32)
    couples = (amount - 1) // 2
    source_of, taker = lengths[1:1 + 2 * couples:2], lengths[2:2 + 2 * couples:2]
    room = jnp.minimum(source_of - 1, reach - taker)
    moved = jax.random.randint(jax.random.fold_in(stream_key, 1), (couples,), 0, 1 << 20) % (room + 1)
    lengths = lengths.at[1:1 + 2 * couples:2].set(source_of - moved).at[2:2 + 2 * couples:2].set(taker + moved)
    return lengths[jax.random.permutation(jax.random.fold_in(stream_key, 2), amount)]


def scatter_about(own_key, extent, width, limit, cuts=(), kind=jnp.bfloat16):
    entries = width * jax.random.normal(own_key, extent, jnp.float32)
    if cuts:
        entries = entries * steps_of(own_key, extent, cuts, -0.22, 0.18)
    return jnp.clip(entries, -limit, limit).astype(kind)


def setup_inputs(seed: int = 0) -> dict:
    seeds = jax.random.split(jax.random.key(seed), 12)
    return {
        "queries": draw_queries(jax.random.fold_in(seeds[11], 71), 0),
        "key_rows": draw_key_rows(jax.random.fold_in(seeds[11], 71), 0),
        "values": scatter_about(seeds[2], (TOKENS, KV_HEADS * HD), 3.0, 16.0, ((0, 16), (1, 2))),
        "doc_ids": jnp.searchsorted(jnp.cumsum(uneven_parts(seeds[3], DOCS, TOKENS, DOC_MOST, 1)), jnp.arange(TOKENS), side="right").astype(jnp.int32),
        "sink_logits": jnp.clip(2.5 + 3.5 * jax.random.uniform(seeds[4], (HEADS,), jnp.float32) ** steps_of(seeds[4], (HEADS,), ((0, 2),), -0.2, 0.2), 2.5, 6.0),
        "residual": scatter_about(seeds[5], (TOKENS, D), 1.0, 6.0, ((0, 16),)),
        "out_weight": scatter_about(seeds[6], (HEADS * HD, D), (HEADS * HD) ** -0.5, 0.1875, ((0, 2),)),
        "norm_gain": jnp.clip(1.0 + 0.18 * jax.random.normal(seeds[7], (D,), jnp.float32), 0.1, 1.9),
        "w_gate": scatter_about(seeds[8], (D, FF), D ** -0.5, 0.125, ((0, 16), (1, 2))),
        "w_up": scatter_about(seeds[9], (D, FF), D ** -0.5, 0.125, ((0, 16), (1, 2))),
        "w_down": scatter_about(seeds[10], (FF, D), FF ** -0.5, 0.078125, ((0, 2), (1, 16))),
    }


def rms_norm(stream, norm_gain):
    floats = stream.astype(jnp.float32)
    scale = lax.rsqrt(lax.optimization_barrier(jnp.mean(floats * floats, axis=-1, keepdims=True)) + 1e-06)
    return floats * scale * norm_gain

def band_rows(tensor, blocks):
    tensor = tensor.reshape((blocks + 1, WINDOW) + tensor.shape[1:])
    return jnp.concatenate([tensor[:-1], tensor[1:]], axis=1)

def sliding(queries, key_rows, values, doc_ids, sink_logits):
    total_rows = queries.shape[0]
    blocks = total_rows // WINDOW
    per_kv = HEADS // KV_HEADS
    pad_rows = jnp.zeros((WINDOW, KV_HEADS * HD), jnp.bfloat16)
    key_band = band_rows(jnp.concatenate([pad_rows, key_rows], axis=0), blocks)
    value_band = band_rows(jnp.concatenate([pad_rows, values], axis=0), blocks)
    doc_band = band_rows(jnp.concatenate([jnp.full((WINDOW,), -1, jnp.int32), doc_ids.astype(jnp.int32)]), blocks)
    key_band = key_band.reshape(blocks, 2 * WINDOW, KV_HEADS, HD).astype(jnp.float32)
    value_band = value_band.reshape(blocks, 2 * WINDOW, KV_HEADS, HD).astype(jnp.float32)
    query_band = queries.reshape(blocks, WINDOW, KV_HEADS, per_kv, HD).astype(jnp.float32)
    scores = jnp.einsum('nqhgd,nkhd->nhgqk', query_band, key_band) * HD ** (-0.5)
    offsets = jnp.arange(WINDOW)[:, None] + WINDOW - jnp.arange(2 * WINDOW)[None, :]
    inside = (offsets >= 0) & (offsets < WINDOW)
    query_docs = doc_ids.reshape(blocks, WINDOW)
    allowed = inside[None] & (query_docs[:, :, None] == doc_band[:, None, :])
    scores = jnp.where(allowed[:, None, None], scores, -1e+30)
    sink_logit = sink_logits.reshape(KV_HEADS, per_kv)[None, :, :, None, None]
    peak = jnp.maximum(lax.optimization_barrier(jnp.max(scores, axis=-1, keepdims=True)), sink_logit)
    raised = jnp.exp(scores - peak)
    denom = lax.optimization_barrier(jnp.sum(raised, axis=-1, keepdims=True)) + jnp.exp(sink_logit - peak)
    weights = (raised / denom).astype(jnp.bfloat16)
    attended = jnp.einsum('nhgqk,nkhd->nqhgd', weights.astype(jnp.float32), value_band)
    return attended.astype(jnp.bfloat16).reshape(total_rows, HEADS * HD)

def grouped_sum(left, right, parts):
    columns = left.shape[1] // parts

    def one(carry, index):
        piece = lax.dynamic_slice_in_dim(left, (index * columns).astype(jnp.int32), columns, 1)
        weight = lax.dynamic_slice_in_dim(right, (index * columns).astype(jnp.int32), columns, 0)
        partial_term = jnp.dot(piece, weight, preferred_element_type=jnp.float32).astype(jnp.bfloat16)
        partial_term = lax.optimization_barrier(partial_term)
        return (carry + partial_term.astype(jnp.float32), None)
    start_acc = jnp.zeros((left.shape[0], right.shape[1]), jnp.float32)
    summed, _ = lax.scan(one, start_acc, jnp.arange(parts, dtype=jnp.int32))
    return summed

def feed_forward(normed, w_gate, w_up, w_down, parts):
    columns = w_gate.shape[1] // parts

    def one(carry, index):
        offset = (index * columns).astype(jnp.int32)
        gate_act = jnp.dot(normed, lax.dynamic_slice_in_dim(w_gate, offset, columns, 1), preferred_element_type=jnp.float32)
        up_act = jnp.dot(normed, lax.dynamic_slice_in_dim(w_up, offset, columns, 1), preferred_element_type=jnp.float32)
        hidden = (jax.nn.silu(gate_act) * up_act).astype(jnp.bfloat16)
        weight = lax.dynamic_slice_in_dim(w_down, offset, columns, 0)
        partial_term = jnp.dot(hidden, weight, preferred_element_type=jnp.float32).astype(jnp.bfloat16)
        partial_term = lax.optimization_barrier(partial_term)
        return (carry + partial_term.astype(jnp.float32), None)
    start_acc = jnp.zeros((normed.shape[0], w_down.shape[1]), jnp.float32)
    summed, _ = lax.scan(one, start_acc, jnp.arange(parts, dtype=jnp.int32))
    return summed

def reference(queries, key_rows, values, doc_ids, sink_logits, residual, out_weight, norm_gain, w_gate, w_up, w_down):
    attended = sliding(queries, key_rows, values, doc_ids, sink_logits)
    mixed_sum = grouped_sum(attended, out_weight, N_TP)
    stream = (residual.astype(jnp.float32) + mixed_sum).astype(jnp.bfloat16)
    normed = rms_norm(stream, norm_gain).astype(jnp.bfloat16)
    mlp_total = feed_forward(normed, w_gate, w_up, w_down, N_TP)
    return (stream.astype(jnp.float32) + mlp_total).astype(jnp.bfloat16)
```

```python
import jax
import jax.numpy as jnp
from jax import lax
from jax.experimental import pallas as pl
from jax.experimental.pallas import tpu as pltpu
from jax.sharding import PartitionSpec as P


HD = 64
WINDOW = 128
INNER = 4
CHUNKS = 2


def from_behind(shard, axis, by):
    size = lax.axis_size(axis)
    pairs = [(i, i + by) for i in range(size) if 0 <= i + by < size]
    return lax.ppermute(shard, axis, pairs)


def rms_norm(stream, norm_gain):
    floats = stream.astype(jnp.float32)
    scale = lax.rsqrt(jnp.mean(floats * floats, axis=-1, keepdims=True) + 1e-06)
    return floats * scale * norm_gain


def band_rows(tensor, blocks):
    tensor = tensor.reshape((blocks + 1, WINDOW) + tensor.shape[1:])
    return jnp.concatenate([tensor[:-1], tensor[1:]], axis=1)


def attend(queries, key_rows, values, doc_ids, sink_logits):
    local_rows = queries.shape[0]
    blocks = local_rows // WINDOW
    kv_local = key_rows.shape[1] // HD
    per_kv = queries.shape[1] // key_rows.shape[1]
    tail_docs = doc_ids[local_rows - WINDOW :] + 1
    width = key_rows.shape[1]
    tail = jnp.concatenate(
        [
            key_rows[local_rows - WINDOW :],
            values[local_rows - WINDOW :],
            jnp.broadcast_to(tail_docs.astype(jnp.bfloat16)[:, None], (WINDOW, 128)),
        ],
        axis=1,
    )
    tail = from_behind(tail, "sp", 1)
    prev_keys, prev_values = tail[:, :width], tail[:, width : 2 * width]
    prev_docs = tail[:, 2 * width].astype(jnp.int32)
    key_band = band_rows(jnp.concatenate([prev_keys, key_rows], axis=0), blocks).reshape(
        blocks, 2 * WINDOW, kv_local, HD
    )
    value_band = band_rows(jnp.concatenate([prev_values, values], axis=0), blocks).reshape(
        blocks, 2 * WINDOW, kv_local, HD
    )
    doc_band = band_rows(jnp.concatenate([prev_docs - 1, doc_ids]), blocks)
    query_band = queries.reshape(blocks, WINDOW, kv_local, per_kv, HD)
    scores = jnp.einsum(
        "nqhgd,nkhd->nhgqk", query_band, key_band, preferred_element_type=jnp.float32
    ) * HD ** (-0.5)
    offsets = jnp.arange(WINDOW)[:, None] + WINDOW - jnp.arange(2 * WINDOW)[None, :]
    inside = (offsets >= 0) & (offsets < WINDOW)
    query_docs = doc_ids.reshape(blocks, WINDOW)
    allowed = inside[None] & (query_docs[:, :, None] == doc_band[:, None, :])
    scores = jnp.where(allowed[:, None, None], scores, -1e30)
    sink_logit = sink_logits.reshape(kv_local, per_kv)[None, :, :, None, None]
    peak = jnp.maximum(jnp.max(scores, axis=-1, keepdims=True), sink_logit)
    raised = jnp.exp(scores - peak)
    denom = jnp.sum(raised, axis=-1, keepdims=True) + jnp.exp(sink_logit - peak)
    weights = (raised / denom).astype(jnp.bfloat16)
    attended = jnp.einsum(
        "nhgqk,nkhd->nqhgd", weights, value_band, preferred_element_type=jnp.float32
    )
    return attended.astype(jnp.bfloat16).reshape(local_rows, queries.shape[1])


def swap(shard, axis, by):
    size = lax.axis_size(axis)
    return lax.ppermute(shard, axis, [(i, i ^ by) for i in range(size)])


def piece_of(tensor, index, axis, pieces):
    size = tensor.shape[axis] // pieces
    return lax.dynamic_slice_in_dim(tensor, index * size, size, axis)


def in_order(mine, others, place, axis):
    size = mine.shape[axis]
    shape = list(mine.shape)
    shape[axis] = size * (len(others) + 1)
    whole = jnp.zeros(shape, mine.dtype)
    for k, shard in enumerate([mine] + others):
        whole = lax.dynamic_update_slice_in_dim(whole, shard, (place ^ k) * size, axis)
    return whole


def on_device(
    queries,
    key_rows,
    values,
    doc_ids,
    sink_logits,
    residual,
    out_weight,
    norm_gain,
    w_gate,
    w_up,
    w_down,
):
    inner = INNER
    outer = lax.axis_size("sp") // inner
    tp = lax.axis_size("tp")
    seat = lax.rem(lax.axis_index("sp"), inner)
    core = lax.axis_index("tp")
    columns = [[row + inner * step for step in range(outer)] for row in range(inner)]

    def gate_up_piece(k):
        return jnp.concatenate(
            [piece_of(w_gate, seat ^ k, 1, inner), piece_of(w_up, seat ^ k, 1, inner)], axis=1
        )

    def down_piece(k):
        return piece_of(w_down, seat ^ k, 0, inner)[None]

    gate_up_pieces = [gate_up_piece(k) for k in range(inner)]
    gate_up_pieces, queries, key_rows, values, w_down = lax.optimization_barrier(
        (gate_up_pieces, queries, key_rows, values, w_down)
    )
    gate_up = in_order(
        gate_up_pieces[0], [swap(gate_up_pieces[k], "sp", k) for k in range(1, inner)], seat, 0
    )
    down = in_order(
        down_piece(0), [swap(down_piece(k), "sp", k) for k in range(1, inner)], seat, 0
    )

    def across(block):
        return lax.all_gather(block, "sp", axis=0, tiled=True, axis_index_groups=columns)

    def flat(gathered):
        return jnp.swapaxes(gathered, 0, 1).reshape(gathered.shape[1], -1)

    part = inner // CHUNKS
    gate_up = across(gate_up)
    downs = []
    for c in range(CHUNKS):
        downs.append(across(down[c * part : (c + 1) * part]))

    attended = attend(queries, key_rows, values, doc_ids, sink_logits)
    mix_term = jnp.dot(attended, out_weight, preferred_element_type=jnp.float32).astype(jnp.bfloat16)
    mixed_sum = piece_of(mix_term, core, 0, tp).astype(jnp.float32)
    for k in range(1, tp):
        mixed_sum += swap(piece_of(mix_term, core ^ k, 0, tp), "tp", k).astype(jnp.float32)
    stream = (piece_of(residual, core, 0, tp).astype(jnp.float32) + mixed_sum).astype(jnp.bfloat16)
    normed = rms_norm(stream, norm_gain).astype(jnp.bfloat16)
    rows, width = normed.shape
    near = jnp.concatenate([normed] + [swap(normed, "sp", k) for k in range(1, inner)], axis=0)
    tokens = jnp.concatenate([near] + [swap(near, "tp", k) for k in range(1, tp)], axis=0)

    acts = jnp.dot(tokens, gate_up, preferred_element_type=jnp.float32)
    units = acts.shape[1] // 2
    hidden = (jax.nn.silu(acts[:, :units]) * acts[:, units:]).astype(jnp.bfloat16)
    block = width // (outer * CHUNKS)
    outs = []
    for c in range(CHUNKS):
        mlp_term = jnp.dot(hidden, lax.optimization_barrier(flat(downs[c])), preferred_element_type=jnp.float32)
        mlp_term = mlp_term.astype(jnp.bfloat16).reshape(tp, inner * rows, width // CHUNKS)
        near_sum = mlp_term[0].astype(jnp.float32)
        for k in range(1, tp):
            near_sum += swap(mlp_term[k], "tp", k).astype(jnp.float32)
        near_sum = near_sum.reshape(inner, rows, width // CHUNKS)
        sends = [near_sum[k].astype(jnp.bfloat16) for k in range(1, inner)]
        total = near_sum[0]
        for k in range(1, inner):
            sent = swap(sends[k - 1], "sp", k)
            total += sent.astype(jnp.float32)
        outs.append(total)
    total = jnp.concatenate(
        [outs[c][:, o * block : (o + 1) * block] for o in range(outer) for c in range(CHUNKS)],
        axis=1,
    )
    out = (stream.astype(jnp.float32) + total).astype(jnp.bfloat16)
    return in_order(out, [swap(out, "tp", k) for k in range(1, tp)], core, 0)


def staged_solution(mesh):
    in_specs = (
        P("sp", "tp"),
        P("sp", "tp"),
        P("sp", "tp"),
        P("sp"),
        P("tp"),
        P("sp", None),
        P("tp", None),
        P(),
        P("sp", "tp"),
        P("sp", "tp"),
        P("tp", "sp"),
    )
    out_specs = P("sp", None)

    return jax.shard_map(
        on_device, mesh=mesh, in_specs=in_specs, out_specs=out_specs, check_vma=False
    )


MESH = pl.DeviceIdType.MESH
GATE_UP, DOWN = 0, 1


def layer_kernel(
    q_hbm, k_hbm, v_hbm, docs_hbm, sink_ref, res_hbm, ow_hbm, gain_ref, gate_hbm, up_hbm, down_hbm,
    o_hbm,
    wgu, wd, xbuf, acts, hid, pbuf, zbuf, rx, rz, own, qbuf, kbuf, vbuf, dbuf, att, ow,
    mix_out, mix_own, mix_in, res, obuf,
    load_sem, halo_s, halo_r, first_s, local_sem, far_s, y_s, sib_s, piece_r, sib_r,
    mix_s, mix_r, tok_s, tok_r, rx_s, rx_r, rz_s, rz_r, out_l, out_s, out_r,
):
    sp, c = lax.axis_index("sp"), lax.axis_index("tp")
    n_sp = lax.axis_size("sp")
    x, y, z = lax.rem(sp, 2), lax.rem(lax.div(sp, 2), 2), lax.div(sp, 4)
    l, h = lax.rem(z, 2), lax.div(z, 2)
    far, near = 2 * (1 - h) + l, 2 * h + 1 - l
    inner, outer = z * (3 - z) == 2, z * (3 - z) == 0
    planes = (z, z + 1 - 2 * h, far, 3 * (1 - l))
    depth, units = gate_hbm.shape[0], gate_hbm.shape[1] // 2
    half_units = units // 2
    rows, width = res_hbm.shape
    half = rows // 2
    blocks = rows // WINDOW
    kv_local = k_hbm.shape[1] // HD
    per_kv = q_hbm.shape[1] // k_hbm.shape[1]
    slab = 4 * depth

    def at(x_, y_, z_, c_):
        return {"sp": 4 * z_ + 2 * y_ + x_, "tp": c_}

    sibling = at(x, y, z, 1 - c)
    x_peer, z_peer = at(1 - x, y, z, c), at(x, y, near, c)

    def remote(src, dst, ss, rs, dev):
        return pltpu.make_async_remote_copy(
            src_ref=src, dst_ref=dst, send_sem=ss, recv_sem=rs, device_id=dev, device_id_type=MESH
        )

    def region(what, k, p):
        if what == GATE_UP:
            return wgu.at[
                pl.ds(pl.multiple_of(p * depth, depth), depth),
                pl.ds(pl.multiple_of(k * units, 128), units),
            ]
        return wd.at[
            pl.ds(pl.multiple_of(k * half_units, 16), half_units),
            pl.ds(pl.multiple_of(p * depth, depth), depth),
        ]

    def source(what, k, xq):
        if what == GATE_UP:
            return (gate_hbm, up_hbm)[k].at[:, pl.ds(pl.multiple_of(xq * units, 128), units)]
        return down_hbm.at[pl.ds(pl.multiple_of(xq * units + k * half_units, 16), half_units), :]

    def first_sends(what, act):
        for k in range(2):
            def copy_to(xq, z_, slot):
                return remote(
                    source(what, k, xq), region(what, k, sp), first_s.at[what, k, slot],
                    piece_r.at[what, sp], at(xq, y, z_, k),
                )

            @pl.when(l == c)
            def _():
                @pl.when(c == k)
                def _():
                    if act == "start":
                        pltpu.make_async_copy(
                            source(what, k, x), region(what, k, sp), local_sem.at[what]
                        ).start()

                @pl.when(c != k)
                def _():
                    getattr(copy_to(x, z, 0), act)()

                getattr(copy_to(1 - x, z, 1), act)()

            @pl.when(l != c)
            def _():
                for i, (dz, ok) in enumerate(((1, z < 3), (-1, z > 0))):
                    @pl.when(ok)
                    def _():
                        for j, xq in enumerate((x, 1 - x)):
                            getattr(copy_to(xq, z + dz, 2 * i + j), act)()

    def wait_piece(what, p):
        reg = region(what, c, p)
        remote(reg, reg, sib_s.at[what, p], piece_r.at[what, p], sibling).wait_recv()

    def far_copy(what, p, i):
        reg = region(what, c, p)
        return remote(reg, reg, far_s.at[what, i], piece_r.at[what, p], at(x, y, far, c))

    def y_copy(what, p, i):
        reg = region(what, c, p)
        return remote(reg, reg, y_s.at[what, i], piece_r.at[what, p], at(x, 1 - y, z, c))

    def sib_copy(what, p):
        reg = region(what, c, p)
        return remote(reg, reg, sib_s.at[what, p], sib_r.at[what, p], sibling)

    def piece(slot, dx, dy=0):
        return 4 * planes[slot] + 2 * (1 - y if dy else y) + (1 - x if dx else x)

    def relay(what, slot, dx):
        p = piece(slot, dx)
        if slot == 0 and dx == 0:
            @pl.when(c == l)
            def _():
                pltpu.make_async_copy(
                    source(what, 0, x), region(what, c, p), local_sem.at[what]
                ).wait()

            @pl.when(c != l)
            def _():
                wait_piece(what, p)
        else:
            wait_piece(what, p)
        if slot == 0:
            far_copy(what, p, dx).start()
        if slot == 3:
            @pl.when(inner)
            def _():
                far_copy(what, p, 2 + dx).start()
        y_copy(what, p, 2 * slot + dx).start()
        sib_copy(what, p).start()

    def relay_both(what, slot):
        for dx in range(2):
            relay(what, slot, dx)

    def relay_y(what, slot):
        for dx in range(2):
            p = piece(slot, dx, 1)
            wait_piece(what, p)
            sib_copy(what, p).start()

    def wait_sib(what, slot):
        for dy in range(2):
            for dx in range(2):
                p = piece(slot, dx, dy)
                reg = region(what, 1 - c, p)
                remote(reg, reg, sib_s.at[what, p], sib_r.at[what, p], sibling).wait_recv()

    own_rows = pl.ds(pl.multiple_of(c * half, half), half)
    sib_rows = pl.ds(pl.multiple_of((1 - c) * half, half), half)
    loads = [
        pltpu.make_async_copy(q_hbm, qbuf, load_sem.at[0]),
        pltpu.make_async_copy(k_hbm, kbuf.at[pl.ds(WINDOW, rows)], load_sem.at[1]),
        pltpu.make_async_copy(v_hbm, vbuf.at[pl.ds(WINDOW, rows)], load_sem.at[2]),
        pltpu.make_async_copy(docs_hbm, dbuf.at[pl.ds(1, blocks)], load_sem.at[3]),
        pltpu.make_async_copy(ow_hbm, ow, load_sem.at[4]),
        pltpu.make_async_copy(res_hbm.at[own_rows], res, load_sem.at[5]),
    ]
    for load in loads:
        load.start()

    tail = pl.ds(rows - WINDOW, WINDOW)
    head = pl.ds(0, WINDOW)
    after = {"sp": lax.rem(sp + 1, n_sp), "tp": c}

    halo = [
        remote(k_hbm.at[tail], kbuf.at[head], halo_s.at[0], halo_r.at[0], after),
        remote(v_hbm.at[tail], vbuf.at[head], halo_s.at[1], halo_r.at[1], after),
        remote(docs_hbm.at[blocks - 1], dbuf.at[0], halo_s.at[2], halo_r.at[2], after),
    ]

    @pl.when(sp < n_sp - 1)
    def _():
        for copy in halo:
            copy.start()

    first_sends(GATE_UP, "start")
    relay(GATE_UP, 0, 0)

    @pl.when(sp == 0)
    def _():
        kbuf[head, :] = jnp.zeros((WINDOW, kbuf.shape[1]), kbuf.dtype)
        vbuf[head, :] = jnp.zeros((WINDOW, vbuf.shape[1]), vbuf.dtype)
        dbuf[0] = jnp.full((1, WINDOW), -1, jnp.int32)

    for load in loads[:4]:
        load.wait()

    def attend_block(n):
        at_rows = pl.ds(pl.multiple_of(n * WINDOW, WINDOW), WINDOW)
        band = pl.ds(pl.multiple_of(n * WINDOW, WINDOW), 2 * WINDOW)
        before_docs, here_docs = dbuf[n], dbuf[n + 1]
        query_docs = jnp.transpose(jnp.broadcast_to(here_docs, (WINDOW, WINDOW)))
        row = lax.broadcasted_iota(jnp.int32, (WINDOW, WINDOW), 0)
        col = lax.broadcasted_iota(jnp.int32, (WINDOW, WINDOW), 1)
        left = (col > row) & (query_docs == before_docs)
        right = (col <= row) & (query_docs == here_docs)
        allowed = jnp.concatenate([left.astype(jnp.int32), right.astype(jnp.int32)], axis=1)
        allowed = jnp.concatenate([allowed] * per_kv, axis=0) != 0
        for j in range(kv_local):
            keys = kbuf[band, j * HD : (j + 1) * HD]
            vals = vbuf[band, j * HD : (j + 1) * HD]
            wide = qbuf[at_rows, j * per_kv * HD : (j + 1) * per_kv * HD]
            query = jnp.concatenate([wide[:, h * HD : (h + 1) * HD] for h in range(per_kv)], axis=0)
            scores = lax.dot_general(
                query, keys, (((1,), (1,)), ((), ())), preferred_element_type=jnp.float32
            ) * HD ** (-0.5)
            scores = jnp.where(allowed, scores, -1e30)
            sink = jnp.concatenate(
                [jnp.full((WINDOW, 1), sink_ref[j * per_kv + h], jnp.float32) for h in range(per_kv)],
                axis=0,
            )
            peak = jnp.maximum(jnp.max(scores, axis=-1, keepdims=True), sink)
            raised = jnp.exp(scores - peak)
            denom = jnp.sum(raised, axis=-1, keepdims=True) + jnp.exp(sink - peak)
            weights = (raised * (1.0 / denom)).astype(jnp.bfloat16)
            mixed = jnp.dot(weights, vals, preferred_element_type=jnp.float32)
            mixed = jnp.concatenate(
                [mixed[h * WINDOW : (h + 1) * WINDOW] for h in range(per_kv)], axis=1
            )
            att[at_rows, j * per_kv * HD : (j + 1) * per_kv * HD] = mixed.astype(jnp.bfloat16)

    def attend_loop(n, carry):
        attend_block(n)
        return carry

    lax.fori_loop(1, blocks, attend_loop, 0)

    @pl.when(sp > 0)
    def _():
        for copy in halo:
            copy.wait_recv()

    lax.fori_loop(0, 1, attend_loop, 0)
    loads[4].wait()

    def project(at_rows, dst):
        def body(i, carry):
            cols = pl.ds(pl.multiple_of(i * 256, 256), 256)
            dst[:, cols] = jnp.dot(
                att[at_rows, :], ow[:, cols], preferred_element_type=jnp.float32
            ).astype(jnp.bfloat16)
            return carry

        lax.fori_loop(0, width // 256, body, 0)

    project(sib_rows, mix_out)
    mix_copy = remote(mix_out, mix_in, mix_s, mix_r, sibling)
    mix_copy.start()
    project(own_rows, mix_own)
    loads[5].wait()
    mix_copy.wait_recv()

    base = 3 * half

    def norm_body(i, carry):
        at_rows = pl.ds(pl.multiple_of(i * 32, 32), 32)
        mixed = mix_own[at_rows, :].astype(jnp.float32) + mix_in[at_rows, :].astype(jnp.float32)
        stream = (res[at_rows, :].astype(jnp.float32) + mixed).astype(jnp.bfloat16)
        res[at_rows, :] = stream
        floats = stream.astype(jnp.float32)
        scale = lax.rsqrt(jnp.mean(floats * floats, axis=-1, keepdims=True) + 1e-06)
        xbuf[pl.ds(pl.multiple_of(base + i * 32, 32), 32), :] = (
            floats * scale * gain_ref[...]
        ).astype(jnp.bfloat16)
        return carry

    chunk = half // 2

    def rows_of(block, i):
        return xbuf.at[pl.ds(block * half + i * chunk, chunk)]

    def token_copy(kind, i):
        src, dst, dev = {
            0: (2, 0, x_peer),
            1: (3, 1, x_peer),
            2: (3, 2, z_peer),
        }[kind]
        return remote(
            rows_of(src, i), rows_of(dst, i), tok_s.at[kind, i], tok_r.at[kind, i], dev
        )

    relay(GATE_UP, 0, 1)
    for i in range(2):
        lax.fori_loop(i * (chunk // 32), (i + 1) * (chunk // 32), norm_body, 0)
        token_copy(1, i).start()
        token_copy(2, i).start()

    @pl.when(inner)
    def _():
        relay_both(GATE_UP, 3)

    relay_both(GATE_UP, 1)
    relay_y(GATE_UP, 0)
    for i in range(2):
        token_copy(2, i).wait_recv()
        token_copy(0, i).start()
    first_sends(DOWN, "start")
    relay(DOWN, 0, 0)
    relay_both(GATE_UP, 2)

    @pl.when(outer)
    def _():
        relay_both(GATE_UP, 3)

    for slot in (1, 3, 2):
        relay_y(GATE_UP, slot)
    relay(DOWN, 0, 1)
    for slot in range(4):
        wait_sib(GATE_UP, slot)
    for i in range(2):
        token_copy(1, i).wait_recv()
        token_copy(0, i).wait_recv()

    pair = 2 * half

    def gate_up(which, lo, hi):
        at_rows = pl.ds(which * pair, pair)

        def body(i, carry):
            cols = pl.ds(pl.multiple_of(i * 256, 256), 256)
            acts[:, cols] = jnp.dot(
                xbuf[at_rows, :], wgu[:, cols], preferred_element_type=jnp.float32
            )
            return carry

        lax.fori_loop(lo, hi, body, 0)

    def activate(which):
        def body(i, carry):
            at_rows = pl.ds(pl.multiple_of(i * 32, 32), 32)
            gate, up = acts[at_rows, :units], acts[at_rows, units:]
            hid[pl.ds(pl.multiple_of(which * pair + i * 32, 32), 32), :] = (
                gate / (1.0 + jnp.exp(-gate)) * up
            ).astype(jnp.bfloat16)
            return carry

        lax.fori_loop(0, pair // 32, body, 0)

    def slab_cols(slot):
        return pl.ds(pl.multiple_of(planes[slot] * slab, slab), slab)

    def x_copy(slot):
        part = pbuf.at[:, slab_cols(slot)]
        return remote(part, rx.at[:, slab_cols(slot)], rx_s.at[planes[slot]], rx_r.at[planes[slot]], x_peer)

    def z_copy(slot):
        part = zbuf.at[:, slab_cols(slot)]
        return remote(part, rz.at[:, slab_cols(slot)], rz_s.at[planes[slot]], rz_r.at[planes[slot]], z_peer)

    def out_copy(slot):
        part = obuf.at[:, slab_cols(slot)]
        dst = o_hbm.at[own_rows, slab_cols(slot)]
        i = planes[slot]
        return (
            pltpu.make_async_copy(part, dst, out_l.at[i]),
            remote(part, dst, out_s.at[i], out_r.at[i], sibling),
        )

    def down_first(slot):
        def body(i, carry):
            cols = pl.ds(pl.multiple_of(planes[slot] * slab + i * 256, 256), 256)
            pbuf[:, cols] = jnp.dot(
                hid[:pair, :], wd[:, cols], preferred_element_type=jnp.float32
            ).astype(jnp.bfloat16)
            return carry

        lax.fori_loop(0, slab // 256, body, 0)
        x_copy(slot).start()

    def down_second(slot):
        def body(i, carry):
            cols = pl.ds(pl.multiple_of(planes[slot] * slab + i * 256, 256), 256)
            part = jnp.dot(hid[pair:, :], wd[:, cols], preferred_element_type=jnp.float32)
            zbuf[:, cols] = part[:half].astype(jnp.bfloat16)
            own[:, cols] = part[half:]
            return carry

        lax.fori_loop(0, slab // 256, body, 0)

    def combine(slot):
        x_copy(slot).wait_recv()

        def body(i, carry):
            cols = pl.ds(pl.multiple_of(planes[slot] * slab + i * 256, 256), 256)
            zbuf[:, cols] = (
                zbuf[:, cols].astype(jnp.float32) + rx[:half, cols].astype(jnp.float32)
            ).astype(jnp.bfloat16)
            return carry

        lax.fori_loop(0, slab // 256, body, 0)
        z_copy(slot).start()

    def finish(slot):
        z_copy(slot).wait_recv()

        def body(i, carry):
            cols = pl.ds(pl.multiple_of(planes[slot] * slab + i * 256, 256), 256)
            total = own[:, cols] + rx[half:, cols].astype(jnp.float32) + rz[:, cols].astype(jnp.float32)
            obuf[:, cols] = (res[:, cols].astype(jnp.float32) + total).astype(jnp.bfloat16)
            return carry

        lax.fori_loop(0, slab // 256, body, 0)
        for copy in out_copy(slot):
            copy.start()

    n_cols = 2 * units // 256
    gate_up(0, 0, n_cols // 2)

    @pl.when(inner)
    def _():
        relay_both(DOWN, 3)

    relay_both(DOWN, 1)
    gate_up(0, n_cols // 2, n_cols)
    activate(0)
    relay_y(DOWN, 0)
    relay_y(DOWN, 1)
    for slot in (0, 1):
        wait_sib(DOWN, slot)
        down_first(slot)
    relay_both(DOWN, 2)

    @pl.when(outer)
    def _():
        relay_both(DOWN, 3)

    gate_up(1, 0, n_cols)
    activate(1)
    for slot in (3, 2):
        relay_y(DOWN, slot)
    for slot in (0, 1):
        down_second(slot)
    for slot in (3, 2):
        wait_sib(DOWN, slot)
        down_first(slot)
    for slot in (0, 1):
        combine(slot)
    for slot in (3, 2):
        down_second(slot)
        combine(slot)
    for slot in (0, 1, 3, 2):
        finish(slot)

    for slot in range(4):
        here, there = out_copy(slot)
        here.wait()
        there.wait()
        x_copy(slot).wait_send()
        z_copy(slot).wait_send()

    @pl.when(sp < n_sp - 1)
    def _():
        for copy in halo:
            copy.wait_send()

    mix_copy.wait_send()
    for kind in range(3):
        for i in range(2):
            token_copy(kind, i).wait_send()
    for what in (GATE_UP, DOWN):
        first_sends(what, "wait_send")
        for slot in range(4):
            for dx in range(2):
                p = piece(slot, dx)
                y_copy(what, p, 2 * slot + dx).wait_send()
                for dy in range(2):
                    sib_copy(what, piece(slot, dx, dy)).wait_send()
        for dx in range(2):
            far_copy(what, piece(0, dx), dx).wait_send()

            @pl.when(inner)
            def _():
                far_copy(what, piece(3, dx), 2 + dx).wait_send()


def fused_on_device(
    queries, key_rows, values, doc_ids, sink_logits, residual, out_weight, norm_gain, w_gate, w_up, w_down
):
    rows, width = residual.shape
    half = rows // 2
    units = w_gate.shape[1] // 2
    pieces = lax.axis_size("sp")
    bf16, f32 = jnp.bfloat16, jnp.float32
    anywhere = pl.BlockSpec(memory_space=pl.ANY)
    dma = pltpu.SemaphoreType.DMA
    docs = doc_ids.reshape(rows // WINDOW, 1, WINDOW)
    return pl.pallas_call(
        layer_kernel,
        out_shape=jax.ShapeDtypeStruct((rows, width), bf16),
        in_specs=[
            anywhere, anywhere, anywhere, anywhere,
            pl.BlockSpec(memory_space=pltpu.SMEM),
            anywhere, anywhere,
            pl.BlockSpec(memory_space=pltpu.VMEM),
            anywhere, anywhere, anywhere,
        ],
        out_specs=anywhere,
        scratch_shapes=[
            pltpu.VMEM((width, 2 * units), bf16),
            pltpu.VMEM((units, width), bf16),
            pltpu.VMEM((4 * half, width), bf16),
            pltpu.VMEM((2 * half, 2 * units), f32),
            pltpu.VMEM((4 * half, units), bf16),
            pltpu.VMEM((2 * half, width), bf16),
            pltpu.VMEM((half, width), bf16),
            pltpu.VMEM((2 * half, width), bf16),
            pltpu.VMEM((half, width), bf16),
            pltpu.VMEM((half, width), f32),
            pltpu.VMEM(queries.shape, bf16),
            pltpu.VMEM((rows + WINDOW, key_rows.shape[1]), bf16),
            pltpu.VMEM((rows + WINDOW, key_rows.shape[1]), bf16),
            pltpu.VMEM((rows // WINDOW + 1, 1, WINDOW), jnp.int32),
            pltpu.VMEM(queries.shape, bf16),
            pltpu.VMEM(out_weight.shape, bf16),
            pltpu.VMEM((half, width), bf16),
            pltpu.VMEM((half, width), bf16),
            pltpu.VMEM((half, width), bf16),
            pltpu.VMEM((half, width), bf16),
            pltpu.VMEM((half, width), bf16),
            dma((6,)), dma((3,)), dma((3,)), dma((2, 2, 4)), dma((2,)), dma((2, 4)), dma((2, 8)),
            dma((2, pieces)), dma((2, pieces)), dma((2, pieces)),
            dma, dma, dma((3, 2)), dma((3, 2)), dma((4,)), dma((4,)), dma((4,)), dma((4,)),
            dma((4,)), dma((4,)), dma((4,)),
        ],
        compiler_params=pltpu.CompilerParams(has_side_effects=True, vmem_limit_bytes=63 * 2**20),
        name="layer",
    )(
        queries, key_rows, values, docs, sink_logits, residual, out_weight,
        norm_gain.reshape(1, width), w_gate, w_up, w_down,
    )


def solution(mesh):
    if (mesh.shape["sp"], mesh.shape["tp"]) != (16, 2):
        return staged_solution(mesh)
    in_specs = (
        P("sp", "tp"), P("sp", "tp"), P("sp", "tp"), P("sp"), P("tp"), P("sp", None), P("tp", None),
        P(), P("sp", "tp"), P("sp", "tp"), P("tp", "sp"),
    )
    return jax.shard_map(
        fused_on_device, mesh=mesh, in_specs=in_specs, out_specs=P("sp", None), check_vma=False
    )
```

```python
import jax
import jax.numpy as jnp
from jax import lax
from jax.experimental import pallas as pl
from jax.experimental.pallas import tpu as pltpu
from jax.sharding import PartitionSpec as P


HD = 64
WINDOW = 128
INNER = 4
CHUNKS = 2


def from_behind(shard, axis, by):
    size = lax.axis_size(axis)
    pairs = [(i, i + by) for i in range(size) if 0 <= i + by < size]
    return lax.ppermute(shard, axis, pairs)


def rms_norm(stream, norm_gain):
    floats = stream.astype(jnp.float32)
    scale = lax.rsqrt(jnp.mean(floats * floats, axis=-1, keepdims=True) + 1e-06)
    return floats * scale * norm_gain


def band_rows(tensor, blocks):
    tensor = tensor.reshape((blocks + 1, WINDOW) + tensor.shape[1:])
    return jnp.concatenate([tensor[:-1], tensor[1:]], axis=1)


def attend(queries, key_rows, values, doc_ids, sink_logits):
    local_rows = queries.shape[0]
    blocks = local_rows // WINDOW
    kv_local = key_rows.shape[1] // HD
    per_kv = queries.shape[1] // key_rows.shape[1]
    tail_docs = doc_ids[local_rows - WINDOW :] + 1
    width = key_rows.shape[1]
    tail = jnp.concatenate(
        [
            key_rows[local_rows - WINDOW :],
            values[local_rows - WINDOW :],
            jnp.broadcast_to(tail_docs.astype(jnp.bfloat16)[:, None], (WINDOW, 128)),
        ],
        axis=1,
    )
    tail = from_behind(tail, "sp", 1)
    prev_keys, prev_values = tail[:, :width], tail[:, width : 2 * width]
    prev_docs = tail[:, 2 * width].astype(jnp.int32)
    key_band = band_rows(jnp.concatenate([prev_keys, key_rows], axis=0), blocks).reshape(
        blocks, 2 * WINDOW, kv_local, HD
    )
    value_band = band_rows(jnp.concatenate([prev_values, values], axis=0), blocks).reshape(
        blocks, 2 * WINDOW, kv_local, HD
    )
    doc_band = band_rows(jnp.concatenate([prev_docs - 1, doc_ids]), blocks)
    query_band = queries.reshape(blocks, WINDOW, kv_local, per_kv, HD)
    scores = jnp.einsum(
        "nqhgd,nkhd->nhgqk", query_band, key_band, preferred_element_type=jnp.float32
    ) * HD ** (-0.5)
    offsets = jnp.arange(WINDOW)[:, None] + WINDOW - jnp.arange(2 * WINDOW)[None, :]
    inside = (offsets >= 0) & (offsets < WINDOW)
    query_docs = doc_ids.reshape(blocks, WINDOW)
    allowed = inside[None] & (query_docs[:, :, None] == doc_band[:, None, :])
    scores = jnp.where(allowed[:, None, None], scores, -1e30)
    sink_logit = sink_logits.reshape(kv_local, per_kv)[None, :, :, None, None]
    peak = jnp.maximum(jnp.max(scores, axis=-1, keepdims=True), sink_logit)
    raised = jnp.exp(scores - peak)
    denom = jnp.sum(raised, axis=-1, keepdims=True) + jnp.exp(sink_logit - peak)
    weights = (raised / denom).astype(jnp.bfloat16)
    attended = jnp.einsum(
        "nhgqk,nkhd->nqhgd", weights, value_band, preferred_element_type=jnp.float32
    )
    return attended.astype(jnp.bfloat16).reshape(local_rows, queries.shape[1])


def swap(shard, axis, by):
    size = lax.axis_size(axis)
    return lax.ppermute(shard, axis, [(i, i ^ by) for i in range(size)])


def piece_of(tensor, index, axis, pieces):
    size = tensor.shape[axis] // pieces
    return lax.dynamic_slice_in_dim(tensor, index * size, size, axis)


def in_order(mine, others, place, axis):
    size = mine.shape[axis]
    shape = list(mine.shape)
    shape[axis] = size * (len(others) + 1)
    whole = jnp.zeros(shape, mine.dtype)
    for k, shard in enumerate([mine] + others):
        whole = lax.dynamic_update_slice_in_dim(whole, shard, (place ^ k) * size, axis)
    return whole


def on_device(
    queries,
    key_rows,
    values,
    doc_ids,
    sink_logits,
    residual,
    out_weight,
    norm_gain,
    w_gate,
    w_up,
    w_down,
):
    inner = INNER
    outer = lax.axis_size("sp") // inner
    tp = lax.axis_size("tp")
    seat = lax.rem(lax.axis_index("sp"), inner)
    core = lax.axis_index("tp")
    columns = [[row + inner * step for step in range(outer)] for row in range(inner)]

    def gate_up_piece(k):
        return jnp.concatenate(
            [piece_of(w_gate, seat ^ k, 1, inner), piece_of(w_up, seat ^ k, 1, inner)], axis=1
        )

    def down_piece(k):
        return piece_of(w_down, seat ^ k, 0, inner)[None]

    gate_up_pieces = [gate_up_piece(k) for k in range(inner)]
    gate_up_pieces, queries, key_rows, values, w_down = lax.optimization_barrier(
        (gate_up_pieces, queries, key_rows, values, w_down)
    )
    gate_up = in_order(
        gate_up_pieces[0], [swap(gate_up_pieces[k], "sp", k) for k in range(1, inner)], seat, 0
    )
    down = in_order(
        down_piece(0), [swap(down_piece(k), "sp", k) for k in range(1, inner)], seat, 0
    )

    def across(block):
        return lax.all_gather(block, "sp", axis=0, tiled=True, axis_index_groups=columns)

    def flat(gathered):
        return jnp.swapaxes(gathered, 0, 1).reshape(gathered.shape[1], -1)

    part = inner // CHUNKS
    gate_up = across(gate_up)
    downs = []
    for c in range(CHUNKS):
        downs.append(across(down[c * part : (c + 1) * part]))

    attended = attend(queries, key_rows, values, doc_ids, sink_logits)
    mix_term = jnp.dot(attended, out_weight, preferred_element_type=jnp.float32).astype(jnp.bfloat16)
    mixed_sum = piece_of(mix_term, core, 0, tp).astype(jnp.float32)
    for k in range(1, tp):
        mixed_sum += swap(piece_of(mix_term, core ^ k, 0, tp), "tp", k).astype(jnp.float32)
    stream = (piece_of(residual, core, 0, tp).astype(jnp.float32) + mixed_sum).astype(jnp.bfloat16)
    normed = rms_norm(stream, norm_gain).astype(jnp.bfloat16)
    rows, width = normed.shape
    near = jnp.concatenate([normed] + [swap(normed, "sp", k) for k in range(1, inner)], axis=0)
    tokens = jnp.concatenate([near] + [swap(near, "tp", k) for k in range(1, tp)], axis=0)

    acts = jnp.dot(tokens, gate_up, preferred_element_type=jnp.float32)
    units = acts.shape[1] // 2
    hidden = (jax.nn.silu(acts[:, :units]) * acts[:, units:]).astype(jnp.bfloat16)
    block = width // (outer * CHUNKS)
    outs = []
    for c in range(CHUNKS):
        mlp_term = jnp.dot(hidden, lax.optimization_barrier(flat(downs[c])), preferred_element_type=jnp.float32)
        mlp_term = mlp_term.astype(jnp.bfloat16).reshape(tp, inner * rows, width // CHUNKS)
        near_sum = mlp_term[0].astype(jnp.float32)
        for k in range(1, tp):
            near_sum += swap(mlp_term[k], "tp", k).astype(jnp.float32)
        near_sum = near_sum.reshape(inner, rows, width // CHUNKS)
        sends = [near_sum[k].astype(jnp.bfloat16) for k in range(1, inner)]
        total = near_sum[0]
        for k in range(1, inner):
            sent = swap(sends[k - 1], "sp", k)
            total += sent.astype(jnp.float32)
        outs.append(total)
    total = jnp.concatenate(
        [outs[c][:, o * block : (o + 1) * block] for o in range(outer) for c in range(CHUNKS)],
        axis=1,
    )
    out = (stream.astype(jnp.float32) + total).astype(jnp.bfloat16)
    return in_order(out, [swap(out, "tp", k) for k in range(1, tp)], core, 0)


def staged_solution(mesh):
    in_specs = (
        P("sp", "tp"),
        P("sp", "tp"),
        P("sp", "tp"),
        P("sp"),
        P("tp"),
        P("sp", None),
        P("tp", None),
        P(),
        P("sp", "tp"),
        P("sp", "tp"),
        P("tp", "sp"),
    )
    out_specs = P("sp", None)

    return jax.shard_map(
        on_device, mesh=mesh, in_specs=in_specs, out_specs=out_specs, check_vma=False
    )


MESH = pl.DeviceIdType.MESH
GATE_UP, DOWN = 0, 1


def layer_kernel(
    q_hbm, k_hbm, v_hbm, docs_hbm, sink_ref, res_hbm, ow_hbm, gain_ref, gate_hbm, up_hbm, down_hbm,
    o_hbm,
    wgu, wd, xbuf, acts, hid, pbuf, zbuf, rx, rz, own, qbuf, kbuf, vbuf, dbuf, att, ow,
    mix_out, mix_own, mix_in, res, obuf,
    load_sem, halo_s, halo_r, first_s, local_sem, far_s, y_s, sib_s, piece_r, sib_r,
    mix_s, mix_r, tok_s, tok_r, rx_s, rx_r, rz_s, rz_r, out_l, out_s, out_r,
):
    sp, c = lax.axis_index("sp"), lax.axis_index("tp")
    n_sp = lax.axis_size("sp")
    x, y, z = lax.rem(sp, 2), lax.rem(lax.div(sp, 2), 2), lax.div(sp, 4)
    l, h = lax.rem(z, 2), lax.div(z, 2)
    far, near = 2 * (1 - h) + l, 2 * h + 1 - l
    mid = lax.div(z * (3 - z), 2)
    inner, outer = mid == 1, mid == 0
    toward, edge = z + 1 - 2 * h, 3 * (1 - l)
    planes = (
        z,
        mid * edge + (1 - mid) * toward,
        far,
        mid * toward + (1 - mid) * edge,
    )
    down_planes = (
        planes[0],
        planes[1],
        mid * toward + (1 - mid) * far,
        mid * far + (1 - mid) * edge,
    )
    depth, units = gate_hbm.shape[0], gate_hbm.shape[1] // 2
    half_units = units // 2
    rows, width = res_hbm.shape
    half = rows // 2
    blocks = rows // WINDOW
    kv_local = k_hbm.shape[1] // HD
    per_kv = q_hbm.shape[1] // k_hbm.shape[1]
    slab = 4 * depth

    def at(x_, y_, z_, c_):
        return {"sp": 4 * z_ + 2 * y_ + x_, "tp": c_}

    sibling = at(x, y, z, 1 - c)
    x_peer, z_peer = at(1 - x, y, z, c), at(x, y, near, c)

    def remote(src, dst, ss, rs, dev):
        return pltpu.make_async_remote_copy(
            src_ref=src, dst_ref=dst, send_sem=ss, recv_sem=rs, device_id=dev, device_id_type=MESH
        )

    def region(what, k, p):
        if what == GATE_UP:
            return wgu.at[
                pl.ds(pl.multiple_of(p * depth, depth), depth),
                pl.ds(pl.multiple_of(k * units, 128), units),
            ]
        return wd.at[
            pl.ds(pl.multiple_of(k * half_units, 16), half_units),
            pl.ds(pl.multiple_of(p * depth, depth), depth),
        ]

    def source(what, k, xq):
        if what == GATE_UP:
            return (gate_hbm, up_hbm)[k].at[:, pl.ds(pl.multiple_of(xq * units, 128), units)]
        return down_hbm.at[pl.ds(pl.multiple_of(xq * units + k * half_units, 16), half_units), :]

    def first_sends(what, act, plane):
        def copy_to(k, xq, z_, slot):
            return remote(
                source(what, k, xq), region(what, k, sp), first_s.at[what, k, slot],
                piece_r.at[what, sp], at(xq, y, z_, k),
            )

        def within():
            for k in range(2):
                getattr(copy_to(k, 1 - x, z, 1), act)()

                @pl.when(c == k)
                def _():
                    if act == "start":
                        pltpu.make_async_copy(
                            source(what, k, x), region(what, k, sp), local_sem.at[what]
                        ).start()

                @pl.when(c != k)
                def _():
                    getattr(copy_to(k, x, z, 0), act)()

        def across(away, j):
            xq, to = (1 - x if j else x), (2 * z - toward if away else toward)
            for k in range(2):
                getattr(copy_to(k, xq, to, 2 * away + j), act)()

        if plane == "own":
            pl.when(l == c)(within)
        elif plane == "away":
            @pl.when(jnp.logical_and(l != c, inner))
            def _():
                across(1, 0)
                across(1, 1)
        else:
            pl.when(l != c)(lambda: across(0, plane == "toward_crossing"))

    def wait_piece(what, p):
        reg = region(what, c, p)
        remote(reg, reg, sib_s.at[what, p], piece_r.at[what, p], sibling).wait_recv()

    def far_copy(what, p, i):
        reg = region(what, c, p)
        return remote(reg, reg, far_s.at[what, i], piece_r.at[what, p], at(x, y, far, c))

    def y_copy(what, p, i):
        reg = region(what, c, p)
        return remote(reg, reg, y_s.at[what, i], piece_r.at[what, p], at(x, 1 - y, z, c))

    def sib_copy(what, p):
        reg = region(what, c, p)
        return remote(reg, reg, sib_s.at[what, p], sib_r.at[what, p], sibling)

    def piece(what, slot, dx, dy=0):
        return 4 * (planes, down_planes)[what][slot] + 2 * (1 - y if dy else y) + (1 - x if dx else x)

    def relay(what, slot, dx, onward=True):
        p = piece(what, slot, dx)
        if slot == 0 and dx == 0:
            @pl.when(c == l)
            def _():
                pltpu.make_async_copy(
                    source(what, 0, x), region(what, c, p), local_sem.at[what]
                ).wait()

            @pl.when(c != l)
            def _():
                wait_piece(what, p)
        else:
            wait_piece(what, p)
        if slot == 0 and onward:
            far_copy(what, p, dx).start()
        if slot == 1:
            @pl.when(inner)
            def _():
                far_copy(what, p, 2 + dx).start()
        y_copy(what, p, 2 * slot + dx).start()
        sib_copy(what, p).start()

    def relay_both(what, slot):
        for dx in range(2):
            relay(what, slot, dx)

    def relay_y(what, slot):
        for dx in range(2):
            p = piece(what, slot, dx, 1)
            wait_piece(what, p)
            sib_copy(what, p).start()

    def wait_sib(what, slot):
        for dy in range(2):
            for dx in range(2):
                p = piece(what, slot, dx, dy)
                reg = region(what, 1 - c, p)
                remote(reg, reg, sib_s.at[what, p], sib_r.at[what, p], sibling).wait_recv()

    greeted = [
        (sibling, None), (at(x, 1 - y, z, c), None), (at(x, y, far, c), None),
        (at(1 - x, y, z, 0), None), (at(1 - x, y, z, 1), None),
        ({"sp": lax.rem(sp + 1, n_sp), "tp": c}, sp < n_sp - 1),
        ({"sp": lax.rem(sp + n_sp - 1, n_sp), "tp": c}, sp > 0),
    ]
    for dz, ok in ((1, z < 3), (-1, z > 0)):
        greeted += [(at(x_, y, z + dz, c_), ok) for x_ in (x, 1 - x) for c_ in range(2)]
    barrier = pltpu.get_barrier_semaphore()
    for dev, ok in greeted:
        def greet():
            pl.semaphore_signal(barrier, inc=1, device_id=dev, device_id_type=MESH)

        if ok is None:
            greet()
        else:
            pl.when(ok)(greet)
    pl.semaphore_wait(barrier, sum(1 if ok is None else ok.astype(jnp.int32) * 1 for _, ok in greeted))

    own_rows = pl.ds(pl.multiple_of(c * half, half), half)
    sib_rows = pl.ds(pl.multiple_of((1 - c) * half, half), half)
    loads = [
        pltpu.make_async_copy(q_hbm, qbuf, load_sem.at[0]),
        pltpu.make_async_copy(k_hbm, kbuf.at[pl.ds(WINDOW, rows)], load_sem.at[1]),
        pltpu.make_async_copy(v_hbm, vbuf.at[pl.ds(WINDOW, rows)], load_sem.at[2]),
        pltpu.make_async_copy(docs_hbm, dbuf.at[pl.ds(1, blocks)], load_sem.at[3]),
        pltpu.make_async_copy(ow_hbm, ow, load_sem.at[4]),
        pltpu.make_async_copy(res_hbm.at[own_rows], res, load_sem.at[5]),
    ]
    for load in loads:
        load.start()

    tail = pl.ds(rows - WINDOW, WINDOW)
    head = pl.ds(0, WINDOW)
    after = {"sp": lax.rem(sp + 1, n_sp), "tp": c}

    halo = [
        remote(k_hbm.at[tail], kbuf.at[head], halo_s.at[0], halo_r.at[0], after),
        remote(v_hbm.at[tail], vbuf.at[head], halo_s.at[1], halo_r.at[1], after),
        remote(docs_hbm.at[blocks - 1], dbuf.at[0], halo_s.at[2], halo_r.at[2], after),
    ]

    @pl.when(sp < n_sp - 1)
    def _():
        for copy in halo:
            copy.start()

    first_sends(GATE_UP, "start", "own")
    first_sends(GATE_UP, "start", "away")

    @pl.when(outer)
    def _():
        first_sends(GATE_UP, "start", "toward")
        first_sends(GATE_UP, "start", "toward_crossing")

    relay(GATE_UP, 0, 0)

    @pl.when(sp == 0)
    def _():
        kbuf[head, :] = jnp.zeros((WINDOW, kbuf.shape[1]), kbuf.dtype)
        vbuf[head, :] = jnp.zeros((WINDOW, vbuf.shape[1]), vbuf.dtype)
        dbuf[0] = jnp.full((1, WINDOW), -1, jnp.int32)

    for load in loads[:4]:
        load.wait()

    def attend_block(n):
        at_rows = pl.ds(pl.multiple_of(n * WINDOW, WINDOW), WINDOW)
        band = pl.ds(pl.multiple_of(n * WINDOW, WINDOW), 2 * WINDOW)
        before_docs, here_docs = dbuf[n], dbuf[n + 1]
        query_docs = jnp.transpose(jnp.broadcast_to(here_docs, (WINDOW, WINDOW)))
        row = lax.broadcasted_iota(jnp.int32, (WINDOW, WINDOW), 0)
        col = lax.broadcasted_iota(jnp.int32, (WINDOW, WINDOW), 1)
        left = (col > row) & (query_docs == before_docs)
        right = (col <= row) & (query_docs == here_docs)
        allowed = jnp.concatenate([left.astype(jnp.int32), right.astype(jnp.int32)], axis=1)
        allowed = jnp.concatenate([allowed] * per_kv, axis=0) != 0
        for j in range(kv_local):
            keys = kbuf[band, j * HD : (j + 1) * HD]
            vals = vbuf[band, j * HD : (j + 1) * HD]
            wide = qbuf[at_rows, j * per_kv * HD : (j + 1) * per_kv * HD]
            query = jnp.concatenate([wide[:, h * HD : (h + 1) * HD] for h in range(per_kv)], axis=0)
            scores = lax.dot_general(
                query, keys, (((1,), (1,)), ((), ())), preferred_element_type=jnp.float32
            ) * HD ** (-0.5)
            scores = jnp.where(allowed, scores, -1e30)
            sink = jnp.concatenate(
                [jnp.full((WINDOW, 1), sink_ref[j * per_kv + h], jnp.float32) for h in range(per_kv)],
                axis=0,
            )
            peak = jnp.maximum(jnp.max(scores, axis=-1, keepdims=True), sink)
            raised = jnp.exp(scores - peak)
            denom = jnp.sum(raised, axis=-1, keepdims=True) + jnp.exp(sink - peak)
            weights = (raised * (1.0 / denom)).astype(jnp.bfloat16)
            mixed = jnp.dot(weights, vals, preferred_element_type=jnp.float32)
            mixed = jnp.concatenate(
                [mixed[h * WINDOW : (h + 1) * WINDOW] for h in range(per_kv)], axis=1
            )
            att[at_rows, j * per_kv * HD : (j + 1) * per_kv * HD] = mixed.astype(jnp.bfloat16)

    def attend_loop(n, carry):
        attend_block(n)
        return carry

    lax.fori_loop(1, blocks, attend_loop, 0)
    relay(GATE_UP, 0, 1)

    @pl.when(inner)
    def _():
        first_sends(GATE_UP, "start", "toward_crossing")
        first_sends(GATE_UP, "start", "toward")

    first_sends(DOWN, "start", "own")

    @pl.when(sp > 0)
    def _():
        for copy in halo:
            copy.wait_recv()

    lax.fori_loop(0, 1, attend_loop, 0)
    loads[4].wait()

    def project(at_rows, dst):
        def body(i, carry):
            cols = pl.ds(pl.multiple_of(i * 256, 256), 256)
            dst[:, cols] = jnp.dot(
                att[at_rows, :], ow[:, cols], preferred_element_type=jnp.float32
            ).astype(jnp.bfloat16)
            return carry

        lax.fori_loop(0, width // 256, body, 0)

    project(sib_rows, mix_out)
    mix_copy = remote(mix_out, mix_in, mix_s, mix_r, sibling)
    mix_copy.start()
    project(own_rows, mix_own)
    loads[5].wait()
    mix_copy.wait_recv()

    base = half

    def norm_body(i, carry):
        at_rows = pl.ds(pl.multiple_of(i * 32, 32), 32)
        mixed = mix_own[at_rows, :].astype(jnp.float32) + mix_in[at_rows, :].astype(jnp.float32)
        stream = (res[at_rows, :].astype(jnp.float32) + mixed).astype(jnp.bfloat16)
        res[at_rows, :] = stream
        floats = stream.astype(jnp.float32)
        scale = lax.rsqrt(jnp.mean(floats * floats, axis=-1, keepdims=True) + 1e-06)
        xbuf[pl.ds(pl.multiple_of(base + i * 32, 32), 32), :] = (
            floats * scale * gain_ref[...]
        ).astype(jnp.bfloat16)
        return carry

    chunk = half // 2

    def rows_of(block, i):
        return xbuf.at[pl.ds(block * half + i * chunk, chunk)]

    def token_copy(kind, i):
        src, dst, dev = {
            0: (3, 2, x_peer),
            1: (1, 0, x_peer),
            2: (1, 3, z_peer),
            3: (0, 2, z_peer),
        }[kind]
        return remote(
            rows_of(src, i), rows_of(dst, i), tok_s.at[kind, i], tok_r.at[kind, i], dev
        )

    pair = 2 * half

    def gate_up(which, slot):
        at_rows = pl.ds(which * pair, pair)
        depths = pl.ds(pl.multiple_of(planes[slot] * slab, slab), slab)

        def body(i, carry):
            cols = pl.ds(pl.multiple_of(i * 256, 256), 256)
            part = jnp.dot(
                xbuf[at_rows, depths], wgu[depths, cols], preferred_element_type=jnp.float32
            )
            acts[at_rows, cols] = part if slot == 0 else acts[at_rows, cols] + part
            return carry

        lax.fori_loop(0, 2 * units // 256, body, 0)

    def gate_up_whole(which, low, high):
        at_rows = pl.ds(which * pair, pair)

        def body(i, carry):
            cols = pl.ds(pl.multiple_of(i * 256, 256), 256)
            acts[at_rows, cols] = jnp.dot(
                xbuf[at_rows, :], wgu[:, cols], preferred_element_type=jnp.float32
            )
            return carry

        lax.fori_loop(low, high, body, 0)

    def activate(which):
        def body(i, carry):
            at_rows = pl.ds(pl.multiple_of(which * pair + i * 32, 32), 32)
            gate, up = acts[at_rows, :units], acts[at_rows, units:]
            hid[at_rows, :] = (gate / (1.0 + jnp.exp(-gate)) * up).astype(jnp.bfloat16)
            return carry

        lax.fori_loop(0, pair // 32, body, 0)

    def slab_cols(slot):
        return pl.ds(pl.multiple_of(down_planes[slot] * slab, slab), slab)

    def x_copy(part, slot):
        i, cols = down_planes[slot], slab_cols(slot)
        dev = z_peer if (part, slot) == (0, 3) else x_peer
        return remote(
            pbuf.at[part, :, cols], rx.at[part, :, cols], rx_s.at[part, i], rx_r.at[part, i], dev
        )

    def z_copy(slot):
        i, cols = down_planes[slot], slab_cols(slot)
        return remote(zbuf.at[:, cols], rz.at[:, cols], rz_s.at[i], rz_r.at[i], z_peer)

    def out_copy(slot):
        part, i = obuf.at[:, slab_cols(slot)], down_planes[slot]
        dst = o_hbm.at[own_rows, slab_cols(slot)]
        return (
            pltpu.make_async_copy(part, dst, out_l.at[i]),
            remote(part, dst, out_s.at[i], out_r.at[i], sibling),
        )

    def over_columns(slot, step):
        def body(i, carry):
            step(pl.ds(pl.multiple_of(down_planes[slot] * slab + i * 256, 256), 256))
            return carry

        lax.fori_loop(0, slab // 256, body, 0)

    def down_first(slot):
        def step(cols):
            part = jnp.dot(hid[:pair, :], wd[:, cols], preferred_element_type=jnp.float32)
            pbuf[1, :, cols] = part[:half].astype(jnp.bfloat16)
            own[:, cols] = part[half:]

        over_columns(slot, step)
        if slot < 3:
            x_copy(1, slot).start()

    def down_second(slot):
        def step(cols):
            part = jnp.dot(hid[pair:, :], wd[:, cols], preferred_element_type=jnp.float32)
            pbuf[0, :, cols] = part[:half].astype(jnp.bfloat16)
            zbuf[:, cols] = part[half:].astype(jnp.bfloat16)

        over_columns(slot, step)
        x_copy(0, slot).start()
        if slot == 3:
            z_copy(slot).start()

    def combine(slot):
        x_copy(0, slot).wait_recv()

        def step(cols):
            mine = zbuf if slot < 3 else pbuf.at[1]
            mine[:, cols] = (
                mine[:, cols].astype(jnp.float32) + rx[0, :, cols].astype(jnp.float32)
            ).astype(jnp.bfloat16)

        over_columns(slot, step)
        (z_copy(slot) if slot < 3 else x_copy(1, slot)).start()

    def finish(slot):
        x_copy(1, slot).wait_recv()
        z_copy(slot).wait_recv()

        def step(cols):
            total = own[:, cols] + rx[1, :, cols].astype(jnp.float32) + rz[:, cols].astype(jnp.float32)
            obuf[:, cols] = (res[:, cols].astype(jnp.float32) + total).astype(jnp.bfloat16)

        over_columns(slot, step)
        for copy in out_copy(slot):
            copy.start()

    def forward_tokens(i, kind):
        token_copy(1 if kind == 3 else 2, i).wait_recv()
        token_copy(kind, i).start()

    def await_tokens(kind):
        for i in range(2):
            token_copy(kind, i).wait_recv()

    def await_diagonal():
        @pl.when(outer)
        def _():
            await_tokens(0)

        @pl.when(inner)
        def _():
            await_tokens(2)
            await_tokens(3)

    def send_tokens(kind, i):
        token_copy(kind, i).start()

    for i in range(2):
        lax.fori_loop(i * (chunk // 32), (i + 1) * (chunk // 32), norm_body, 0)
        token_copy(1, i).start()

    @pl.when(outer)
    def _():
        send_tokens(2, 0)
        send_tokens(2, 1)

    relay(DOWN, 0, 0, onward=False)

    @pl.when(outer)
    def _():
        relay(DOWN, 0, 1, onward=False)
        relay_both(GATE_UP, 2)

    relay_y(GATE_UP, 0)
    relay_both(GATE_UP, 1)

    @pl.when(inner)
    def _():
        send_tokens(2, 0)
        relay_both(GATE_UP, 2)
        relay_y(GATE_UP, 1)
        relay(GATE_UP, 3, 1)
        send_tokens(2, 1)
        relay(DOWN, 0, 1, onward=False)
        await_tokens(1)

    @pl.when(outer)
    def _():
        relay_y(GATE_UP, 2)
        for plane in ("toward_crossing", "toward"):
            first_sends(DOWN, "start", plane)
        forward_tokens(0, 3)
        forward_tokens(1, 3)
        forward_tokens(0, 0)
        relay_y(GATE_UP, 1)
        relay(GATE_UP, 3, 0)
        relay(GATE_UP, 3, 1)

    wait_sib(GATE_UP, 0)
    gate_up(0, 0)

    @pl.when(inner)
    def _():
        relay(GATE_UP, 3, 0)
        relay_y(GATE_UP, 2)
        for plane in ("toward_crossing", "toward"):
            first_sends(DOWN, "start", plane)

    @pl.when(outer)
    def _():
        forward_tokens(1, 0)

    wait_sib(GATE_UP, 1)
    gate_up(0, 1)
    wait_sib(GATE_UP, 2)
    gate_up(0, 2)
    first_sends(DOWN, "start", "away")
    for dx in range(2):
        far_copy(DOWN, piece(DOWN, 0, dx), dx).start()

    @pl.when(inner)
    def _():
        relay_both(DOWN, 1)

    relay_y(GATE_UP, 3)
    relay_y(DOWN, 0)
    wait_sib(GATE_UP, 3)
    gate_up(0, 3)
    activate(0)
    wait_sib(DOWN, 0)
    down_first(0)

    @pl.when(outer)
    def _():
        relay_both(DOWN, 1)
        relay_both(DOWN, 2)

    await_diagonal()
    gate_up_whole(1, 0, 8)

    @pl.when(inner)
    def _():
        relay_both(DOWN, 2)

    relay_both(DOWN, 3)
    gate_up_whole(1, 8, 2 * units // 256)
    activate(1)
    down_second(0)
    relay_y(DOWN, 1)
    wait_sib(DOWN, 1)
    down_second(1)
    down_first(1)
    relay_y(DOWN, 2)
    combine(0)
    wait_sib(DOWN, 2)
    down_second(2)
    down_first(2)
    combine(1)
    relay_y(DOWN, 3)
    wait_sib(DOWN, 3)
    down_second(3)
    down_first(3)
    combine(2)
    combine(3)
    for slot in range(4):
        finish(slot)

    for slot in range(4):
        for copy in out_copy(slot):
            copy.wait()
        x_copy(0, slot).wait_send()
        x_copy(1, slot).wait_send()
        z_copy(slot).wait_send()

    @pl.when(sp < n_sp - 1)
    def _():
        for copy in halo:
            copy.wait_send()

    mix_copy.wait_send()
    for i in range(2):
        token_copy(1, i).wait_send()
        token_copy(2, i).wait_send()

        @pl.when(outer)
        def _():
            token_copy(0, i).wait_send()
            token_copy(3, i).wait_send()
    for what in (GATE_UP, DOWN):
        first_sends(what, "wait_send", "own")
        for plane in ("away", "toward", "toward_crossing"):
            first_sends(what, "wait_send", plane)
        for slot in range(4):
            for dx in range(2):
                p = piece(what, slot, dx)
                y_copy(what, p, 2 * slot + dx).wait_send()
                for dy in range(2):
                    sib_copy(what, piece(what, slot, dx, dy)).wait_send()
        for dx in range(2):
            far_copy(what, piece(what, 0, dx), dx).wait_send()

            @pl.when(inner)
            def _():
                far_copy(what, piece(what, 1, dx), 2 + dx).wait_send()


def fused_on_device(
    queries, key_rows, values, doc_ids, sink_logits, residual, out_weight, norm_gain, w_gate, w_up, w_down
):
    rows, width = residual.shape
    half = rows // 2
    units = w_gate.shape[1] // 2
    pieces = lax.axis_size("sp")
    bf16, f32 = jnp.bfloat16, jnp.float32
    anywhere = pl.BlockSpec(memory_space=pl.ANY)
    dma = pltpu.SemaphoreType.DMA
    docs = doc_ids.reshape(rows // WINDOW, 1, WINDOW)
    return pl.pallas_call(
        layer_kernel,
        out_shape=jax.ShapeDtypeStruct((rows, width), bf16),
        in_specs=[
            anywhere, anywhere, anywhere, anywhere,
            pl.BlockSpec(memory_space=pltpu.SMEM),
            anywhere, anywhere,
            pl.BlockSpec(memory_space=pltpu.VMEM),
            anywhere, anywhere, anywhere,
        ],
        out_specs=anywhere,
        scratch_shapes=[
            pltpu.VMEM((width, 2 * units), bf16),
            pltpu.VMEM((units, width), bf16),
            pltpu.VMEM((4 * half, width), bf16),
            pltpu.VMEM((4 * half, 2 * units), f32),
            pltpu.VMEM((4 * half, units), bf16),
            pltpu.VMEM((2, half, width), bf16),
            pltpu.VMEM((half, width), bf16),
            pltpu.VMEM((2, half, width), bf16),
            pltpu.VMEM((half, width), bf16),
            pltpu.VMEM((half, width), f32),
            pltpu.VMEM(queries.shape, bf16),
            pltpu.VMEM((rows + WINDOW, key_rows.shape[1]), bf16),
            pltpu.VMEM((rows + WINDOW, key_rows.shape[1]), bf16),
            pltpu.VMEM((rows // WINDOW + 1, 1, WINDOW), jnp.int32),
            pltpu.VMEM(queries.shape, bf16),
            pltpu.VMEM(out_weight.shape, bf16),
            pltpu.VMEM((half, width), bf16),
            pltpu.VMEM((half, width), bf16),
            pltpu.VMEM((half, width), bf16),
            pltpu.VMEM((half, width), bf16),
            pltpu.VMEM((half, width), bf16),
            dma((6,)), dma((3,)), dma((3,)), dma((2, 2, 4)), dma((2,)), dma((2, 4)), dma((2, 8)),
            dma((2, pieces)), dma((2, pieces)), dma((2, pieces)),
            dma, dma, dma((4, 2)), dma((4, 2)), dma((2, 4)), dma((2, 4)), dma((4,)), dma((4,)),
            dma((4,)), dma((4,)), dma((4,)),
        ],
        compiler_params=pltpu.CompilerParams(has_side_effects=True, collective_id=0, vmem_limit_bytes=63 * 2**20),
        name="layer",
    )(
        queries, key_rows, values, docs, sink_logits, residual, out_weight,
        norm_gain.reshape(1, width), w_gate, w_up, w_down,
    )


def solution(mesh):
    if (mesh.shape["sp"], mesh.shape["tp"]) != (16, 2):
        return staged_solution(mesh)
    in_specs = (
        P("sp", "tp"), P("sp", "tp"), P("sp", "tp"), P("sp"), P("tp"), P("sp", None), P("tp", None),
        P(), P("sp", "tp"), P("sp", "tp"), P("tp", "sp"),
    )
    return jax.shard_map(
        fused_on_device, mesh=mesh, in_specs=in_specs, out_specs=P("sp", None), check_vma=False
    )
```

```python
import jax
import jax.numpy as jnp
from jax import lax
from jax.experimental import pallas as pl
from jax.experimental.pallas import tpu as pltpu
from jax.sharding import PartitionSpec as P


HD = 64
WINDOW = 128
INNER = 4
CHUNKS = 2


def from_behind(shard, axis, by):
    size = lax.axis_size(axis)
    pairs = [(i, i + by) for i in range(size) if 0 <= i + by < size]
    return lax.ppermute(shard, axis, pairs)


def rms_norm(stream, norm_gain):
    floats = stream.astype(jnp.float32)
    scale = lax.rsqrt(jnp.mean(floats * floats, axis=-1, keepdims=True) + 1e-06)
    return floats * scale * norm_gain


def band_rows(tensor, blocks):
    tensor = tensor.reshape((blocks + 1, WINDOW) + tensor.shape[1:])
    return jnp.concatenate([tensor[:-1], tensor[1:]], axis=1)


def attend(queries, key_rows, values, doc_ids, sink_logits):
    local_rows = queries.shape[0]
    blocks = local_rows // WINDOW
    kv_local = key_rows.shape[1] // HD
    per_kv = queries.shape[1] // key_rows.shape[1]
    tail_docs = doc_ids[local_rows - WINDOW :] + 1
    width = key_rows.shape[1]
    tail = jnp.concatenate(
        [
            key_rows[local_rows - WINDOW :],
            values[local_rows - WINDOW :],
            jnp.broadcast_to(tail_docs.astype(jnp.bfloat16)[:, None], (WINDOW, 128)),
        ],
        axis=1,
    )
    tail = from_behind(tail, "sp", 1)
    prev_keys, prev_values = tail[:, :width], tail[:, width : 2 * width]
    prev_docs = tail[:, 2 * width].astype(jnp.int32)
    key_band = band_rows(jnp.concatenate([prev_keys, key_rows], axis=0), blocks).reshape(
        blocks, 2 * WINDOW, kv_local, HD
    )
    value_band = band_rows(jnp.concatenate([prev_values, values], axis=0), blocks).reshape(
        blocks, 2 * WINDOW, kv_local, HD
    )
    doc_band = band_rows(jnp.concatenate([prev_docs - 1, doc_ids]), blocks)
    query_band = queries.reshape(blocks, WINDOW, kv_local, per_kv, HD)
    scores = jnp.einsum(
        "nqhgd,nkhd->nhgqk", query_band, key_band, preferred_element_type=jnp.float32
    ) * HD ** (-0.5)
    offsets = jnp.arange(WINDOW)[:, None] + WINDOW - jnp.arange(2 * WINDOW)[None, :]
    inside = (offsets >= 0) & (offsets < WINDOW)
    query_docs = doc_ids.reshape(blocks, WINDOW)
    allowed = inside[None] & (query_docs[:, :, None] == doc_band[:, None, :])
    scores = jnp.where(allowed[:, None, None], scores, -1e30)
    sink_logit = sink_logits.reshape(kv_local, per_kv)[None, :, :, None, None]
    peak = jnp.maximum(jnp.max(scores, axis=-1, keepdims=True), sink_logit)
    raised = jnp.exp(scores - peak)
    denom = jnp.sum(raised, axis=-1, keepdims=True) + jnp.exp(sink_logit - peak)
    weights = (raised / denom).astype(jnp.bfloat16)
    attended = jnp.einsum(
        "nhgqk,nkhd->nqhgd", weights, value_band, preferred_element_type=jnp.float32
    )
    return attended.astype(jnp.bfloat16).reshape(local_rows, queries.shape[1])


def swap(shard, axis, by):
    size = lax.axis_size(axis)
    return lax.ppermute(shard, axis, [(i, i ^ by) for i in range(size)])


def piece_of(tensor, index, axis, pieces):
    size = tensor.shape[axis] // pieces
    return lax.dynamic_slice_in_dim(tensor, index * size, size, axis)


def in_order(mine, others, place, axis):
    size = mine.shape[axis]
    shape = list(mine.shape)
    shape[axis] = size * (len(others) + 1)
    whole = jnp.zeros(shape, mine.dtype)
    for k, shard in enumerate([mine] + others):
        whole = lax.dynamic_update_slice_in_dim(whole, shard, (place ^ k) * size, axis)
    return whole


def on_device(
    queries,
    key_rows,
    values,
    doc_ids,
    sink_logits,
    residual,
    out_weight,
    norm_gain,
    w_gate,
    w_up,
    w_down,
):
    inner = INNER
    outer = lax.axis_size("sp") // inner
    tp = lax.axis_size("tp")
    seat = lax.rem(lax.axis_index("sp"), inner)
    core = lax.axis_index("tp")
    columns = [[row + inner * step for step in range(outer)] for row in range(inner)]

    def gate_up_piece(k):
        return jnp.concatenate(
            [piece_of(w_gate, seat ^ k, 1, inner), piece_of(w_up, seat ^ k, 1, inner)], axis=1
        )

    def down_piece(k):
        return piece_of(w_down, seat ^ k, 0, inner)[None]

    gate_up_pieces = [gate_up_piece(k) for k in range(inner)]
    gate_up_pieces, queries, key_rows, values, w_down = lax.optimization_barrier(
        (gate_up_pieces, queries, key_rows, values, w_down)
    )
    gate_up = in_order(
        gate_up_pieces[0], [swap(gate_up_pieces[k], "sp", k) for k in range(1, inner)], seat, 0
    )
    down = in_order(
        down_piece(0), [swap(down_piece(k), "sp", k) for k in range(1, inner)], seat, 0
    )

    def across(block):
        return lax.all_gather(block, "sp", axis=0, tiled=True, axis_index_groups=columns)

    def flat(gathered):
        return jnp.swapaxes(gathered, 0, 1).reshape(gathered.shape[1], -1)

    part = inner // CHUNKS
    gate_up = across(gate_up)
    downs = []
    for c in range(CHUNKS):
        downs.append(across(down[c * part : (c + 1) * part]))

    attended = attend(queries, key_rows, values, doc_ids, sink_logits)
    mix_term = jnp.dot(attended, out_weight, preferred_element_type=jnp.float32).astype(jnp.bfloat16)
    mixed_sum = piece_of(mix_term, core, 0, tp).astype(jnp.float32)
    for k in range(1, tp):
        mixed_sum += swap(piece_of(mix_term, core ^ k, 0, tp), "tp", k).astype(jnp.float32)
    stream = (piece_of(residual, core, 0, tp).astype(jnp.float32) + mixed_sum).astype(jnp.bfloat16)
    normed = rms_norm(stream, norm_gain).astype(jnp.bfloat16)
    rows, width = normed.shape
    near = jnp.concatenate([normed] + [swap(normed, "sp", k) for k in range(1, inner)], axis=0)
    tokens = jnp.concatenate([near] + [swap(near, "tp", k) for k in range(1, tp)], axis=0)

    acts = jnp.dot(tokens, gate_up, preferred_element_type=jnp.float32)
    units = acts.shape[1] // 2
    hidden = (jax.nn.silu(acts[:, :units]) * acts[:, units:]).astype(jnp.bfloat16)
    block = width // (outer * CHUNKS)
    outs = []
    for c in range(CHUNKS):
        mlp_term = jnp.dot(hidden, lax.optimization_barrier(flat(downs[c])), preferred_element_type=jnp.float32)
        mlp_term = mlp_term.astype(jnp.bfloat16).reshape(tp, inner * rows, width // CHUNKS)
        near_sum = mlp_term[0].astype(jnp.float32)
        for k in range(1, tp):
            near_sum += swap(mlp_term[k], "tp", k).astype(jnp.float32)
        near_sum = near_sum.reshape(inner, rows, width // CHUNKS)
        sends = [near_sum[k].astype(jnp.bfloat16) for k in range(1, inner)]
        total = near_sum[0]
        for k in range(1, inner):
            sent = swap(sends[k - 1], "sp", k)
            total += sent.astype(jnp.float32)
        outs.append(total)
    total = jnp.concatenate(
        [outs[c][:, o * block : (o + 1) * block] for o in range(outer) for c in range(CHUNKS)],
        axis=1,
    )
    out = (stream.astype(jnp.float32) + total).astype(jnp.bfloat16)
    return in_order(out, [swap(out, "tp", k) for k in range(1, tp)], core, 0)


def staged_solution(mesh):
    in_specs = (
        P("sp", "tp"),
        P("sp", "tp"),
        P("sp", "tp"),
        P("sp"),
        P("tp"),
        P("sp", None),
        P("tp", None),
        P(),
        P("sp", "tp"),
        P("sp", "tp"),
        P("tp", "sp"),
    )
    out_specs = P("sp", None)

    return jax.shard_map(
        on_device, mesh=mesh, in_specs=in_specs, out_specs=out_specs, check_vma=False
    )


MESH = pl.DeviceIdType.MESH
GATE_UP, DOWN = 0, 1


def layer_kernel(
    q_hbm, k_hbm, v_hbm, docs_hbm, sink_ref, res_hbm, ow_hbm, gain_ref, gate_hbm, up_hbm, down_hbm,
    o_hbm,
    wgu, wd, xbuf, acts, hid, pbuf, zbuf, rx, rz, own, qbuf, kbuf, vbuf, dbuf, att, ow,
    mix_out, mix_own, mix_in, res, obuf,
    load_sem, halo_s, halo_r, first_s, local_sem, far_s, y_s, sib_s, piece_r, sib_r,
    mix_s, mix_r, tok_s, tok_r, rx_s, rx_r, rz_s, rz_r, out_l, out_s, out_r,
):
    sp, c = lax.axis_index("sp"), lax.axis_index("tp")
    n_sp = lax.axis_size("sp")
    x, y, z = lax.rem(sp, 2), lax.rem(lax.div(sp, 2), 2), lax.div(sp, 4)
    l, h = lax.rem(z, 2), lax.div(z, 2)
    far, near = 2 * (1 - h) + l, 2 * h + 1 - l
    mid = lax.div(z * (3 - z), 2)
    inner, outer = mid == 1, mid == 0
    toward, edge = z + 1 - 2 * h, 3 * (1 - l)
    planes = (
        z,
        mid * edge + (1 - mid) * toward,
        far,
        mid * toward + (1 - mid) * edge,
    )
    down_planes = (
        planes[0],
        planes[1],
        mid * toward + (1 - mid) * far,
        mid * far + (1 - mid) * edge,
    )
    depth, units = gate_hbm.shape[0], gate_hbm.shape[1] // 2
    half_units = units // 2
    rows, width = res_hbm.shape
    half = rows // 2
    blocks = rows // WINDOW
    kv_local = k_hbm.shape[1] // HD
    per_kv = q_hbm.shape[1] // k_hbm.shape[1]
    slab = 4 * depth

    def at(x_, y_, z_, c_):
        return {"sp": 4 * z_ + 2 * y_ + x_, "tp": c_}

    sibling = at(x, y, z, 1 - c)
    x_peer, z_peer = at(1 - x, y, z, c), at(x, y, near, c)

    def remote(src, dst, ss, rs, dev):
        return pltpu.make_async_remote_copy(
            src_ref=src, dst_ref=dst, send_sem=ss, recv_sem=rs, device_id=dev, device_id_type=MESH
        )

    def region(what, k, p):
        if what == GATE_UP:
            return wgu.at[
                pl.ds(pl.multiple_of(p * depth, depth), depth),
                pl.ds(pl.multiple_of(k * units, 128), units),
            ]
        return wd.at[
            pl.ds(pl.multiple_of(k * half_units, 16), half_units),
            pl.ds(pl.multiple_of(p * depth, depth), depth),
        ]

    def source(what, k, xq):
        if what == GATE_UP:
            return (gate_hbm, up_hbm)[k].at[:, pl.ds(pl.multiple_of(xq * units, 128), units)]
        return down_hbm.at[pl.ds(pl.multiple_of(xq * units + k * half_units, 16), half_units), :]

    def first_sends(what, act, plane):
        def copy_to(k, xq, z_, slot):
            return remote(
                source(what, k, xq), region(what, k, sp), first_s.at[what, k, slot],
                piece_r.at[what, sp], at(xq, y, z_, k),
            )

        def within():
            for k in range(2):
                getattr(copy_to(k, 1 - x, z, 1), act)()

                @pl.when(c == k)
                def _():
                    if act == "start":
                        pltpu.make_async_copy(
                            source(what, k, x), region(what, k, sp), local_sem.at[what]
                        ).start()

                @pl.when(c != k)
                def _():
                    getattr(copy_to(k, x, z, 0), act)()

        def across(away, j):
            xq, to = (1 - x if j else x), (2 * z - toward if away else toward)
            for k in range(2):
                getattr(copy_to(k, xq, to, 2 * away + j), act)()

        if plane == "own":
            pl.when(l == c)(within)
        elif plane == "away":
            @pl.when(jnp.logical_and(l != c, inner))
            def _():
                across(1, 0)
                across(1, 1)
        else:
            pl.when(l != c)(lambda: across(0, plane == "toward_crossing"))

    def wait_piece(what, p):
        reg = region(what, c, p)
        remote(reg, reg, sib_s.at[what, p], piece_r.at[what, p], sibling).wait_recv()

    def far_copy(what, p, i):
        reg = region(what, c, p)
        return remote(reg, reg, far_s.at[what, i], piece_r.at[what, p], at(x, y, far, c))

    def y_copy(what, p, i):
        reg = region(what, c, p)
        return remote(reg, reg, y_s.at[what, i], piece_r.at[what, p], at(x, 1 - y, z, c))

    def sib_copy(what, p):
        reg = region(what, c, p)
        return remote(reg, reg, sib_s.at[what, p], sib_r.at[what, p], sibling)

    def piece(what, slot, dx, dy=0):
        return 4 * (planes, down_planes)[what][slot] + 2 * (1 - y if dy else y) + (1 - x if dx else x)

    def relay(what, slot, dx, onward=True):
        p = piece(what, slot, dx)
        if slot == 0 and dx == 0:
            @pl.when(c == l)
            def _():
                pltpu.make_async_copy(
                    source(what, 0, x), region(what, c, p), local_sem.at[what]
                ).wait()

            @pl.when(c != l)
            def _():
                wait_piece(what, p)
        else:
            wait_piece(what, p)
        if slot == 0 and onward:
            far_copy(what, p, dx).start()
        if slot == 1:
            @pl.when(inner)
            def _():
                far_copy(what, p, 2 + dx).start()
        y_copy(what, p, 2 * slot + dx).start()
        sib_copy(what, p).start()

    def relay_both(what, slot):
        for dx in range(2):
            relay(what, slot, dx)

    def relay_y(what, slot):
        for dx in range(2):
            p = piece(what, slot, dx, 1)
            wait_piece(what, p)
            sib_copy(what, p).start()

    def wait_sib(what, slot):
        for dy in range(2):
            for dx in range(2):
                p = piece(what, slot, dx, dy)
                reg = region(what, 1 - c, p)
                remote(reg, reg, sib_s.at[what, p], sib_r.at[what, p], sibling).wait_recv()

    greeted = [
        (sibling, None), (at(x, 1 - y, z, c), None), (at(x, y, far, c), None),
        (at(1 - x, y, z, 0), None), (at(1 - x, y, z, 1), None),
        ({"sp": lax.rem(sp + 1, n_sp), "tp": c}, sp < n_sp - 1),
        ({"sp": lax.rem(sp + n_sp - 1, n_sp), "tp": c}, sp > 0),
    ]
    for dz, ok in ((1, z < 3), (-1, z > 0)):
        greeted += [(at(x_, y, z + dz, c_), ok) for x_ in (x, 1 - x) for c_ in range(2)]
    barrier = pltpu.get_barrier_semaphore()
    for dev, ok in greeted:
        def greet():
            pl.semaphore_signal(barrier, inc=1, device_id=dev, device_id_type=MESH)

        if ok is None:
            greet()
        else:
            pl.when(ok)(greet)
    pl.semaphore_wait(barrier, sum(1 if ok is None else ok.astype(jnp.int32) * 1 for _, ok in greeted))

    own_rows = pl.ds(pl.multiple_of(c * half, half), half)
    sib_rows = pl.ds(pl.multiple_of((1 - c) * half, half), half)
    loads = [
        pltpu.make_async_copy(q_hbm, qbuf, load_sem.at[0]),
        pltpu.make_async_copy(k_hbm, kbuf.at[pl.ds(WINDOW, rows)], load_sem.at[1]),
        pltpu.make_async_copy(v_hbm, vbuf.at[pl.ds(WINDOW, rows)], load_sem.at[2]),
        pltpu.make_async_copy(docs_hbm, dbuf.at[pl.ds(1, blocks)], load_sem.at[3]),
        pltpu.make_async_copy(ow_hbm, ow, load_sem.at[4]),
        pltpu.make_async_copy(res_hbm.at[own_rows], res, load_sem.at[5]),
    ]
    for load in loads:
        load.start()

    tail = pl.ds(rows - WINDOW, WINDOW)
    head = pl.ds(0, WINDOW)
    after = {"sp": lax.rem(sp + 1, n_sp), "tp": c}

    halo = [
        remote(k_hbm.at[tail], kbuf.at[head], halo_s.at[0], halo_r.at[0], after),
        remote(v_hbm.at[tail], vbuf.at[head], halo_s.at[1], halo_r.at[1], after),
        remote(docs_hbm.at[blocks - 1], dbuf.at[0], halo_s.at[2], halo_r.at[2], after),
    ]

    @pl.when(sp < n_sp - 1)
    def _():
        for copy in halo:
            copy.start()

    first_sends(GATE_UP, "start", "own")
    first_sends(GATE_UP, "start", "away")

    @pl.when(outer)
    def _():
        first_sends(GATE_UP, "start", "toward")
        first_sends(GATE_UP, "start", "toward_crossing")

    relay(GATE_UP, 0, 0)

    @pl.when(sp == 0)
    def _():
        kbuf[head, :] = jnp.zeros((WINDOW, kbuf.shape[1]), kbuf.dtype)
        vbuf[head, :] = jnp.zeros((WINDOW, vbuf.shape[1]), vbuf.dtype)
        dbuf[0] = jnp.full((1, WINDOW), -1, jnp.int32)

    for load in loads[:4]:
        load.wait()

    def attend_block(n):
        at_rows = pl.ds(pl.multiple_of(n * WINDOW, WINDOW), WINDOW)
        band = pl.ds(pl.multiple_of(n * WINDOW, WINDOW), 2 * WINDOW)
        before_docs, here_docs = dbuf[n], dbuf[n + 1]
        query_docs = jnp.transpose(jnp.broadcast_to(here_docs, (WINDOW, WINDOW)))
        row = lax.broadcasted_iota(jnp.int32, (WINDOW, WINDOW), 0)
        col = lax.broadcasted_iota(jnp.int32, (WINDOW, WINDOW), 1)
        left = (col > row) & (query_docs == before_docs)
        right = (col <= row) & (query_docs == here_docs)
        allowed = jnp.concatenate([left.astype(jnp.int32), right.astype(jnp.int32)], axis=1)
        allowed = jnp.concatenate([allowed] * per_kv, axis=0) != 0
        for j in range(kv_local):
            keys = kbuf[band, j * HD : (j + 1) * HD]
            vals = vbuf[band, j * HD : (j + 1) * HD]
            wide = qbuf[at_rows, j * per_kv * HD : (j + 1) * per_kv * HD]
            query = jnp.concatenate([wide[:, h * HD : (h + 1) * HD] for h in range(per_kv)], axis=0)
            scores = lax.dot_general(
                query, keys, (((1,), (1,)), ((), ())), preferred_element_type=jnp.float32
            ) * HD ** (-0.5)
            scores = jnp.where(allowed, scores, -1e30)
            sink = jnp.concatenate(
                [jnp.full((WINDOW, 1), sink_ref[j * per_kv + h], jnp.float32) for h in range(per_kv)],
                axis=0,
            )
            peak = jnp.maximum(jnp.max(scores, axis=-1, keepdims=True), sink)
            raised = jnp.exp(scores - peak)
            denom = jnp.sum(raised, axis=-1, keepdims=True) + jnp.exp(sink - peak)
            weights = (raised * (1.0 / denom)).astype(jnp.bfloat16)
            mixed = jnp.dot(weights, vals, preferred_element_type=jnp.float32)
            mixed = jnp.concatenate(
                [mixed[h * WINDOW : (h + 1) * WINDOW] for h in range(per_kv)], axis=1
            )
            att[at_rows, j * per_kv * HD : (j + 1) * per_kv * HD] = mixed.astype(jnp.bfloat16)

    def attend_loop(n, carry):
        attend_block(n)
        return carry

    lax.fori_loop(1, blocks, attend_loop, 0)
    relay(GATE_UP, 0, 1)

    @pl.when(inner)
    def _():
        first_sends(GATE_UP, "start", "toward_crossing")
        first_sends(GATE_UP, "start", "toward")

    first_sends(DOWN, "start", "own")

    @pl.when(sp > 0)
    def _():
        for copy in halo:
            copy.wait_recv()

    lax.fori_loop(0, 1, attend_loop, 0)
    loads[4].wait()

    def project(at_rows, dst):
        def body(i, carry):
            cols = pl.ds(pl.multiple_of(i * 256, 256), 256)
            dst[:, cols] = jnp.dot(
                att[at_rows, :], ow[:, cols], preferred_element_type=jnp.float32
            ).astype(jnp.bfloat16)
            return carry

        lax.fori_loop(0, width // 256, body, 0)

    project(sib_rows, mix_out)
    mix_copy = remote(mix_out, mix_in, mix_s, mix_r, sibling)
    mix_copy.start()
    project(own_rows, mix_own)
    loads[5].wait()
    mix_copy.wait_recv()

    base = half

    def norm_body(i, carry):
        at_rows = pl.ds(pl.multiple_of(i * 32, 32), 32)
        mixed = mix_own[at_rows, :].astype(jnp.float32) + mix_in[at_rows, :].astype(jnp.float32)
        stream = (res[at_rows, :].astype(jnp.float32) + mixed).astype(jnp.bfloat16)
        res[at_rows, :] = stream
        floats = stream.astype(jnp.float32)
        scale = lax.rsqrt(jnp.mean(floats * floats, axis=-1, keepdims=True) + 1e-06)
        xbuf[pl.ds(pl.multiple_of(base + i * 32, 32), 32), :] = (
            floats * scale * gain_ref[...]
        ).astype(jnp.bfloat16)
        return carry

    chunk = half // 2

    def rows_of(block, i):
        return xbuf.at[pl.ds(block * half + i * chunk, chunk)]

    def token_copy(kind, i):
        src, dst, dev = {
            0: (3, 2, x_peer),
            1: (1, 0, x_peer),
            2: (1, 3, z_peer),
            3: (0, 2, z_peer),
        }[kind]
        return remote(
            rows_of(src, i), rows_of(dst, i), tok_s.at[kind, i], tok_r.at[kind, i], dev
        )

    pair = 2 * half

    def gate_up(which, slot):
        at_rows = pl.ds(which * pair, pair)
        depths = pl.ds(pl.multiple_of(planes[slot] * slab, slab), slab)

        def body(i, carry):
            cols = pl.ds(pl.multiple_of(i * 256, 256), 256)
            part = jnp.dot(
                xbuf[at_rows, depths], wgu[depths, cols], preferred_element_type=jnp.float32
            )
            acts[at_rows, cols] = part if slot == 0 else acts[at_rows, cols] + part
            return carry

        lax.fori_loop(0, 2 * units // 256, body, 0)

    def gate_up_whole(which, low, high):
        at_rows = pl.ds(which * pair, pair)

        def body(i, carry):
            cols = pl.ds(pl.multiple_of(i * 256, 256), 256)
            acts[at_rows, cols] = jnp.dot(
                xbuf[at_rows, :], wgu[:, cols], preferred_element_type=jnp.float32
            )
            return carry

        lax.fori_loop(low, high, body, 0)

    def activate(which):
        def body(i, carry):
            at_rows = pl.ds(pl.multiple_of(which * pair + i * 32, 32), 32)
            gate, up = acts[at_rows, :units], acts[at_rows, units:]
            hid[at_rows, :] = (gate / (1.0 + jnp.exp(-gate)) * up).astype(jnp.bfloat16)
            return carry

        lax.fori_loop(0, pair // 32, body, 0)

    def slab_cols(slot):
        return pl.ds(pl.multiple_of(down_planes[slot] * slab, slab), slab)

    def x_copy(part, slot):
        i, cols = down_planes[slot], slab_cols(slot)
        dev = z_peer if (part, slot) == (0, 3) else x_peer
        return remote(
            pbuf.at[part, :, cols], rx.at[part, :, cols], rx_s.at[part, i], rx_r.at[part, i], dev
        )

    def z_copy(slot):
        i, cols = down_planes[slot], slab_cols(slot)
        return remote(zbuf.at[:, cols], rz.at[:, cols], rz_s.at[i], rz_r.at[i], z_peer)

    def out_copy(slot):
        part, i = obuf.at[:, slab_cols(slot)], down_planes[slot]
        dst = o_hbm.at[own_rows, slab_cols(slot)]
        return (
            pltpu.make_async_copy(part, dst, out_l.at[i]),
            remote(part, dst, out_s.at[i], out_r.at[i], sibling),
        )

    def over_columns(slot, step):
        def body(i, carry):
            step(pl.ds(pl.multiple_of(down_planes[slot] * slab + i * 256, 256), 256))
            return carry

        lax.fori_loop(0, slab // 256, body, 0)

    def down_first(slot):
        def step(cols):
            part = jnp.dot(hid[:pair, :], wd[:, cols], preferred_element_type=jnp.float32)
            pbuf[1, :, cols] = part[:half].astype(jnp.bfloat16)
            own[:, cols] = part[half:]

        over_columns(slot, step)
        if slot < 3:
            x_copy(1, slot).start()

    def down_second(slot):
        def step(cols):
            part = jnp.dot(hid[pair:, :], wd[:, cols], preferred_element_type=jnp.float32)
            pbuf[0, :, cols] = part[:half].astype(jnp.bfloat16)
            zbuf[:, cols] = part[half:].astype(jnp.bfloat16)

        over_columns(slot, step)
        x_copy(0, slot).start()
        if slot == 3:
            z_copy(slot).start()

    def combine(slot):
        x_copy(0, slot).wait_recv()

        def step(cols):
            mine = zbuf if slot < 3 else pbuf.at[1]
            mine[:, cols] = (
                mine[:, cols].astype(jnp.float32) + rx[0, :, cols].astype(jnp.float32)
            ).astype(jnp.bfloat16)

        over_columns(slot, step)
        (z_copy(slot) if slot < 3 else x_copy(1, slot)).start()

    def finish(slot):
        x_copy(1, slot).wait_recv()
        z_copy(slot).wait_recv()

        def step(cols):
            total = own[:, cols] + rx[1, :, cols].astype(jnp.float32) + rz[:, cols].astype(jnp.float32)
            obuf[:, cols] = (res[:, cols].astype(jnp.float32) + total).astype(jnp.bfloat16)

        over_columns(slot, step)
        for copy in out_copy(slot):
            copy.start()

    def forward_tokens(i, kind):
        token_copy(1 if kind == 3 else 2, i).wait_recv()
        token_copy(kind, i).start()

    def await_tokens(kind):
        for i in range(2):
            token_copy(kind, i).wait_recv()

    def await_diagonal():
        @pl.when(outer)
        def _():
            await_tokens(0)

        @pl.when(inner)
        def _():
            token_copy(2, 0).wait_recv()
            token_copy(3, 0).wait_recv()
            token_copy(0, 1).wait_recv()

    def send_tokens(kind, i):
        token_copy(kind, i).start()

    for i in range(2):
        lax.fori_loop(i * (chunk // 32), (i + 1) * (chunk // 32), norm_body, 0)
        token_copy(1, i).start()

    @pl.when(outer)
    def _():
        send_tokens(2, 0)
        send_tokens(2, 1)

    relay(DOWN, 0, 0, onward=False)

    @pl.when(outer)
    def _():
        relay(DOWN, 0, 1, onward=False)
        relay_both(GATE_UP, 2)

    relay_y(GATE_UP, 0)
    relay_both(GATE_UP, 1)

    @pl.when(inner)
    def _():
        send_tokens(2, 0)
        relay_both(GATE_UP, 2)
        relay_y(GATE_UP, 1)
        relay(GATE_UP, 3, 1)
        send_tokens(2, 1)
        relay(DOWN, 0, 1, onward=False)
        await_tokens(1)
        forward_tokens(1, 0)

    @pl.when(outer)
    def _():
        relay_y(GATE_UP, 2)
        for plane in ("toward_crossing", "toward"):
            first_sends(DOWN, "start", plane)
        forward_tokens(0, 3)
        token_copy(1, 1).wait_recv()
        forward_tokens(0, 0)
        relay_y(GATE_UP, 1)
        relay(GATE_UP, 3, 0)
        relay(GATE_UP, 3, 1)

    wait_sib(GATE_UP, 0)
    gate_up(0, 0)

    @pl.when(inner)
    def _():
        relay(GATE_UP, 3, 0)
        relay_y(GATE_UP, 2)
        for plane in ("away", "toward_crossing", "toward"):
            first_sends(DOWN, "start", plane)

    @pl.when(outer)
    def _():
        forward_tokens(1, 0)

    wait_sib(GATE_UP, 1)
    gate_up(0, 1)
    for dx in range(2):
        far_copy(DOWN, piece(DOWN, 0, dx), dx).start()
    wait_sib(GATE_UP, 2)
    gate_up(0, 2)

    @pl.when(inner)
    def _():
        relay_both(DOWN, 1)

    relay_y(GATE_UP, 3)
    relay_y(DOWN, 0)
    wait_sib(GATE_UP, 3)
    gate_up(0, 3)

    @pl.when(outer)
    def _():
        relay_both(DOWN, 1)

    activate(0)
    wait_sib(DOWN, 0)
    down_first(0)

    @pl.when(inner)
    def _():
        relay_y(DOWN, 1)

    await_diagonal()
    gate_up_whole(1, 0, 4)

    @pl.when(inner)
    def _():
        wait_sib(DOWN, 1)
        down_first(1)

    @pl.when(outer)
    def _():
        relay_both(DOWN, 2)

    gate_up_whole(1, 4, 8)

    @pl.when(inner)
    def _():
        relay_both(DOWN, 2)

    gate_up_whole(1, 8, 2 * units // 256)
    activate(1)
    down_second(0)
    relay_both(DOWN, 3)

    @pl.when(outer)
    def _():
        relay_y(DOWN, 1)
        wait_sib(DOWN, 1)

    down_second(1)
    relay_y(DOWN, 2)
    combine(0)
    wait_sib(DOWN, 2)
    down_second(2)

    @pl.when(outer)
    def _():
        down_first(1)

    down_first(2)
    relay_y(DOWN, 3)
    wait_sib(DOWN, 3)
    down_second(3)
    combine(1)
    down_first(3)
    combine(2)
    combine(3)
    for slot in range(4):
        finish(slot)

    for slot in range(4):
        for copy in out_copy(slot):
            copy.wait()
        x_copy(0, slot).wait_send()
        x_copy(1, slot).wait_send()
        z_copy(slot).wait_send()

    @pl.when(sp < n_sp - 1)
    def _():
        for copy in halo:
            copy.wait_send()

    mix_copy.wait_send()
    for i in range(2):
        token_copy(1, i).wait_send()
        token_copy(2, i).wait_send()
    token_copy(0, 1).wait_send()

    @pl.when(outer)
    def _():
        token_copy(0, 0).wait_send()
        token_copy(3, 0).wait_send()

    for what in (GATE_UP, DOWN):
        first_sends(what, "wait_send", "own")
        for plane in ("away", "toward", "toward_crossing"):
            first_sends(what, "wait_send", plane)
        for slot in range(4):
            for dx in range(2):
                p = piece(what, slot, dx)
                y_copy(what, p, 2 * slot + dx).wait_send()
                for dy in range(2):
                    sib_copy(what, piece(what, slot, dx, dy)).wait_send()
        for dx in range(2):
            far_copy(what, piece(what, 0, dx), dx).wait_send()

            @pl.when(inner)
            def _():
                far_copy(what, piece(what, 1, dx), 2 + dx).wait_send()


def fused_on_device(
    queries, key_rows, values, doc_ids, sink_logits, residual, out_weight, norm_gain, w_gate, w_up, w_down
):
    rows, width = residual.shape
    half = rows // 2
    units = w_gate.shape[1] // 2
    pieces = lax.axis_size("sp")
    bf16, f32 = jnp.bfloat16, jnp.float32
    anywhere = pl.BlockSpec(memory_space=pl.ANY)
    dma = pltpu.SemaphoreType.DMA
    docs = doc_ids.reshape(rows // WINDOW, 1, WINDOW)
    return pl.pallas_call(
        layer_kernel,
        out_shape=jax.ShapeDtypeStruct((rows, width), bf16),
        in_specs=[
            anywhere, anywhere, anywhere, anywhere,
            pl.BlockSpec(memory_space=pltpu.SMEM),
            anywhere, anywhere,
            pl.BlockSpec(memory_space=pltpu.VMEM),
            anywhere, anywhere, anywhere,
        ],
        out_specs=anywhere,
        scratch_shapes=[
            pltpu.VMEM((width, 2 * units), bf16),
            pltpu.VMEM((units, width), bf16),
            pltpu.VMEM((4 * half, width), bf16),
            pltpu.VMEM((4 * half, 2 * units), f32),
            pltpu.VMEM((4 * half, units), bf16),
            pltpu.VMEM((2, half, width), bf16),
            pltpu.VMEM((half, width), bf16),
            pltpu.VMEM((2, half, width), bf16),
            pltpu.VMEM((half, width), bf16),
            pltpu.VMEM((half, width), f32),
            pltpu.VMEM(queries.shape, bf16),
            pltpu.VMEM((rows + WINDOW, key_rows.shape[1]), bf16),
            pltpu.VMEM((rows + WINDOW, key_rows.shape[1]), bf16),
            pltpu.VMEM((rows // WINDOW + 1, 1, WINDOW), jnp.int32),
            pltpu.VMEM(queries.shape, bf16),
            pltpu.VMEM(out_weight.shape, bf16),
            pltpu.VMEM((half, width), bf16),
            pltpu.VMEM((half, width), bf16),
            pltpu.VMEM((half, width), bf16),
            pltpu.VMEM((half, width), bf16),
            pltpu.VMEM((half, width), bf16),
            dma((6,)), dma((3,)), dma((3,)), dma((2, 2, 4)), dma((2,)), dma((2, 4)), dma((2, 8)),
            dma((2, pieces)), dma((2, pieces)), dma((2, pieces)),
            dma, dma, dma((4, 2)), dma((4, 2)), dma((2, 4)), dma((2, 4)), dma((4,)), dma((4,)),
            dma((4,)), dma((4,)), dma((4,)),
        ],
        compiler_params=pltpu.CompilerParams(has_side_effects=True, collective_id=0, vmem_limit_bytes=63 * 2**20),
        name="layer",
    )(
        queries, key_rows, values, docs, sink_logits, residual, out_weight,
        norm_gain.reshape(1, width), w_gate, w_up, w_down,
    )


def solution(mesh):
    if (mesh.shape["sp"], mesh.shape["tp"]) != (16, 2):
        return staged_solution(mesh)
    in_specs = (
        P("sp", "tp"), P("sp", "tp"), P("sp", "tp"), P("sp"), P("tp"), P("sp", None), P("tp", None),
        P(), P("sp", "tp"), P("sp", "tp"), P("tp", "sp"),
    )
    return jax.shard_map(
        fused_on_device, mesh=mesh, in_specs=in_specs, out_specs=P("sp", None), check_vma=False
    )
```

```python
import jax
import jax.numpy as jnp
from jax import lax
from jax.experimental import pallas as pl
from jax.experimental.pallas import tpu as pltpu
from jax.sharding import PartitionSpec as P


HD = 64
WINDOW = 128
INNER = 4
CHUNKS = 2


def from_behind(shard, axis, by):
    size = lax.axis_size(axis)
    pairs = [(i, i + by) for i in range(size) if 0 <= i + by < size]
    return lax.ppermute(shard, axis, pairs)


def rms_norm(stream, norm_gain):
    floats = stream.astype(jnp.float32)
    scale = lax.rsqrt(jnp.mean(floats * floats, axis=-1, keepdims=True) + 1e-06)
    return floats * scale * norm_gain


def band_rows(tensor, blocks):
    tensor = tensor.reshape((blocks + 1, WINDOW) + tensor.shape[1:])
    return jnp.concatenate([tensor[:-1], tensor[1:]], axis=1)


def attend(queries, key_rows, values, doc_ids, sink_logits):
    local_rows = queries.shape[0]
    blocks = local_rows // WINDOW
    kv_local = key_rows.shape[1] // HD
    per_kv = queries.shape[1] // key_rows.shape[1]
    tail_docs = doc_ids[local_rows - WINDOW :] + 1
    width = key_rows.shape[1]
    tail = jnp.concatenate(
        [
            key_rows[local_rows - WINDOW :],
            values[local_rows - WINDOW :],
            jnp.broadcast_to(tail_docs.astype(jnp.bfloat16)[:, None], (WINDOW, 128)),
        ],
        axis=1,
    )
    tail = from_behind(tail, "sp", 1)
    prev_keys, prev_values = tail[:, :width], tail[:, width : 2 * width]
    prev_docs = tail[:, 2 * width].astype(jnp.int32)
    key_band = band_rows(jnp.concatenate([prev_keys, key_rows], axis=0), blocks).reshape(
        blocks, 2 * WINDOW, kv_local, HD
    )
    value_band = band_rows(jnp.concatenate([prev_values, values], axis=0), blocks).reshape(
        blocks, 2 * WINDOW, kv_local, HD
    )
    doc_band = band_rows(jnp.concatenate([prev_docs - 1, doc_ids]), blocks)
    query_band = queries.reshape(blocks, WINDOW, kv_local, per_kv, HD)
    scores = jnp.einsum(
        "nqhgd,nkhd->nhgqk", query_band, key_band, preferred_element_type=jnp.float32
    ) * HD ** (-0.5)
    offsets = jnp.arange(WINDOW)[:, None] + WINDOW - jnp.arange(2 * WINDOW)[None, :]
    inside = (offsets >= 0) & (offsets < WINDOW)
    query_docs = doc_ids.reshape(blocks, WINDOW)
    allowed = inside[None] & (query_docs[:, :, None] == doc_band[:, None, :])
    scores = jnp.where(allowed[:, None, None], scores, -1e30)
    sink_logit = sink_logits.reshape(kv_local, per_kv)[None, :, :, None, None]
    peak = jnp.maximum(jnp.max(scores, axis=-1, keepdims=True), sink_logit)
    raised = jnp.exp(scores - peak)
    denom = jnp.sum(raised, axis=-1, keepdims=True) + jnp.exp(sink_logit - peak)
    weights = (raised / denom).astype(jnp.bfloat16)
    attended = jnp.einsum(
        "nhgqk,nkhd->nqhgd", weights, value_band, preferred_element_type=jnp.float32
    )
    return attended.astype(jnp.bfloat16).reshape(local_rows, queries.shape[1])


def swap(shard, axis, by):
    size = lax.axis_size(axis)
    return lax.ppermute(shard, axis, [(i, i ^ by) for i in range(size)])


def piece_of(tensor, index, axis, pieces):
    size = tensor.shape[axis] // pieces
    return lax.dynamic_slice_in_dim(tensor, index * size, size, axis)


def in_order(mine, others, place, axis):
    size = mine.shape[axis]
    shape = list(mine.shape)
    shape[axis] = size * (len(others) + 1)
    whole = jnp.zeros(shape, mine.dtype)
    for k, shard in enumerate([mine] + others):
        whole = lax.dynamic_update_slice_in_dim(whole, shard, (place ^ k) * size, axis)
    return whole


def on_device(
    queries,
    key_rows,
    values,
    doc_ids,
    sink_logits,
    residual,
    out_weight,
    norm_gain,
    w_gate,
    w_up,
    w_down,
):
    inner = INNER
    outer = lax.axis_size("sp") // inner
    tp = lax.axis_size("tp")
    seat = lax.rem(lax.axis_index("sp"), inner)
    core = lax.axis_index("tp")
    columns = [[row + inner * step for step in range(outer)] for row in range(inner)]

    def gate_up_piece(k):
        return jnp.concatenate(
            [piece_of(w_gate, seat ^ k, 1, inner), piece_of(w_up, seat ^ k, 1, inner)], axis=1
        )

    def down_piece(k):
        return piece_of(w_down, seat ^ k, 0, inner)[None]

    gate_up_pieces = [gate_up_piece(k) for k in range(inner)]
    gate_up_pieces, queries, key_rows, values, w_down = lax.optimization_barrier(
        (gate_up_pieces, queries, key_rows, values, w_down)
    )
    gate_up = in_order(
        gate_up_pieces[0], [swap(gate_up_pieces[k], "sp", k) for k in range(1, inner)], seat, 0
    )
    down = in_order(
        down_piece(0), [swap(down_piece(k), "sp", k) for k in range(1, inner)], seat, 0
    )

    def across(block):
        return lax.all_gather(block, "sp", axis=0, tiled=True, axis_index_groups=columns)

    def flat(gathered):
        return jnp.swapaxes(gathered, 0, 1).reshape(gathered.shape[1], -1)

    part = inner // CHUNKS
    gate_up = across(gate_up)
    downs = []
    for c in range(CHUNKS):
        downs.append(across(down[c * part : (c + 1) * part]))

    attended = attend(queries, key_rows, values, doc_ids, sink_logits)
    mix_term = jnp.dot(attended, out_weight, preferred_element_type=jnp.float32).astype(jnp.bfloat16)
    mixed_sum = piece_of(mix_term, core, 0, tp).astype(jnp.float32)
    for k in range(1, tp):
        mixed_sum += swap(piece_of(mix_term, core ^ k, 0, tp), "tp", k).astype(jnp.float32)
    stream = (piece_of(residual, core, 0, tp).astype(jnp.float32) + mixed_sum).astype(jnp.bfloat16)
    normed = rms_norm(stream, norm_gain).astype(jnp.bfloat16)
    rows, width = normed.shape
    near = jnp.concatenate([normed] + [swap(normed, "sp", k) for k in range(1, inner)], axis=0)
    tokens = jnp.concatenate([near] + [swap(near, "tp", k) for k in range(1, tp)], axis=0)

    acts = jnp.dot(tokens, gate_up, preferred_element_type=jnp.float32)
    units = acts.shape[1] // 2
    hidden = (jax.nn.silu(acts[:, :units]) * acts[:, units:]).astype(jnp.bfloat16)
    block = width // (outer * CHUNKS)
    outs = []
    for c in range(CHUNKS):
        mlp_term = jnp.dot(hidden, lax.optimization_barrier(flat(downs[c])), preferred_element_type=jnp.float32)
        mlp_term = mlp_term.astype(jnp.bfloat16).reshape(tp, inner * rows, width // CHUNKS)
        near_sum = mlp_term[0].astype(jnp.float32)
        for k in range(1, tp):
            near_sum += swap(mlp_term[k], "tp", k).astype(jnp.float32)
        near_sum = near_sum.reshape(inner, rows, width // CHUNKS)
        sends = [near_sum[k].astype(jnp.bfloat16) for k in range(1, inner)]
        total = near_sum[0]
        for k in range(1, inner):
            sent = swap(sends[k - 1], "sp", k)
            total += sent.astype(jnp.float32)
        outs.append(total)
    total = jnp.concatenate(
        [outs[c][:, o * block : (o + 1) * block] for o in range(outer) for c in range(CHUNKS)],
        axis=1,
    )
    out = (stream.astype(jnp.float32) + total).astype(jnp.bfloat16)
    return in_order(out, [swap(out, "tp", k) for k in range(1, tp)], core, 0)


def staged_solution(mesh):
    in_specs = (
        P("sp", "tp"),
        P("sp", "tp"),
        P("sp", "tp"),
        P("sp"),
        P("tp"),
        P("sp", None),
        P("tp", None),
        P(),
        P("sp", "tp"),
        P("sp", "tp"),
        P("tp", "sp"),
    )
    out_specs = P("sp", None)

    return jax.shard_map(
        on_device, mesh=mesh, in_specs=in_specs, out_specs=out_specs, check_vma=False
    )


MESH = pl.DeviceIdType.MESH
GATE_UP, DOWN = 0, 1


def layer_kernel(
    q_hbm, k_hbm, v_hbm, docs_hbm, sink_ref, res_hbm, ow_hbm, gain_ref, gate_hbm, up_hbm, down_hbm,
    o_hbm,
    wgu, wd, xbuf, acts, hid, pbuf, zbuf, rx, rz, own, qbuf, kbuf, vbuf, dbuf, att, ow,
    mix_out, mix_own, mix_in, res, obuf,
    load_sem, halo_s, halo_r, first_s, local_sem, far_s, y_s, sib_s, piece_r, sib_r,
    mix_s, mix_r, tok_s, tok_r, rx_s, rx_r, rz_s, rz_r, out_l, out_s, out_r,
):
    sp, c = lax.axis_index("sp"), lax.axis_index("tp")
    n_sp = lax.axis_size("sp")
    x, y, z = lax.rem(sp, 2), lax.rem(lax.div(sp, 2), 2), lax.div(sp, 4)
    l, h = lax.rem(z, 2), lax.div(z, 2)
    far, near = 2 * (1 - h) + l, 2 * h + 1 - l
    mid = lax.div(z * (3 - z), 2)
    inner, outer = mid == 1, mid == 0
    toward, edge = z + 1 - 2 * h, 3 * (1 - l)
    planes = (
        z,
        mid * edge + (1 - mid) * toward,
        far,
        mid * toward + (1 - mid) * edge,
    )
    down_planes = (
        planes[0],
        planes[1],
        mid * toward + (1 - mid) * far,
        mid * far + (1 - mid) * edge,
    )
    depth, units = gate_hbm.shape[0], gate_hbm.shape[1] // 2
    half_units = units // 2
    rows, width = res_hbm.shape
    half = rows // 2
    blocks = rows // WINDOW
    kv_local = k_hbm.shape[1] // HD
    per_kv = q_hbm.shape[1] // k_hbm.shape[1]
    slab = 4 * depth

    def at(x_, y_, z_, c_):
        return {"sp": 4 * z_ + 2 * y_ + x_, "tp": c_}

    sibling = at(x, y, z, 1 - c)
    x_peer, z_peer = at(1 - x, y, z, c), at(x, y, near, c)

    def remote(src, dst, ss, rs, dev):
        return pltpu.make_async_remote_copy(
            src_ref=src, dst_ref=dst, send_sem=ss, recv_sem=rs, device_id=dev, device_id_type=MESH
        )

    def region(what, k, p):
        if what == GATE_UP:
            return wgu.at[
                pl.ds(pl.multiple_of(p * depth, depth), depth),
                pl.ds(pl.multiple_of(k * units, 128), units),
            ]
        return wd.at[
            pl.ds(pl.multiple_of(k * half_units, 16), half_units),
            pl.ds(pl.multiple_of(p * depth, depth), depth),
        ]

    def source(what, k, xq):
        if what == GATE_UP:
            return (gate_hbm, up_hbm)[k].at[:, pl.ds(pl.multiple_of(xq * units, 128), units)]
        return down_hbm.at[pl.ds(pl.multiple_of(xq * units + k * half_units, 16), half_units), :]

    def first_sends(what, act, plane):
        def copy_to(k, xq, z_, slot):
            return remote(
                source(what, k, xq), region(what, k, sp), first_s.at[what, k, slot],
                piece_r.at[what, sp], at(xq, y, z_, k),
            )

        def within():
            for k in range(2):
                getattr(copy_to(k, 1 - x, z, 1), act)()

                @pl.when(c == k)
                def _():
                    if act == "start":
                        pltpu.make_async_copy(
                            source(what, k, x), region(what, k, sp), local_sem.at[what]
                        ).start()

                @pl.when(c != k)
                def _():
                    getattr(copy_to(k, x, z, 0), act)()

        def across(away, j):
            xq, to = (1 - x if j else x), (2 * z - toward if away else toward)
            for k in range(2):
                getattr(copy_to(k, xq, to, 2 * away + j), act)()

        if plane == "own":
            pl.when(l == c)(within)
        elif plane == "away":
            @pl.when(jnp.logical_and(l != c, inner))
            def _():
                across(1, 0)
                across(1, 1)
        else:
            pl.when(l != c)(lambda: across(0, plane == "toward_crossing"))

    def wait_piece(what, p):
        reg = region(what, c, p)
        remote(reg, reg, sib_s.at[what, p], piece_r.at[what, p], sibling).wait_recv()

    def far_copy(what, p, i):
        reg = region(what, c, p)
        return remote(reg, reg, far_s.at[what, i], piece_r.at[what, p], at(x, y, far, c))

    def y_copy(what, p, i):
        reg = region(what, c, p)
        return remote(reg, reg, y_s.at[what, i], piece_r.at[what, p], at(x, 1 - y, z, c))

    def sib_copy(what, p):
        reg = region(what, c, p)
        return remote(reg, reg, sib_s.at[what, p], sib_r.at[what, p], sibling)

    def piece(what, slot, dx, dy=0):
        return 4 * (planes, down_planes)[what][slot] + 2 * (1 - y if dy else y) + (1 - x if dx else x)

    def relay(what, slot, dx, onward=True):
        p = piece(what, slot, dx)
        if slot == 0 and dx == 0:
            @pl.when(c == l)
            def _():
                pltpu.make_async_copy(
                    source(what, 0, x), region(what, c, p), local_sem.at[what]
                ).wait()

            @pl.when(c != l)
            def _():
                wait_piece(what, p)
        else:
            wait_piece(what, p)
        if slot == 0 and onward:
            far_copy(what, p, dx).start()
        if slot == 1:
            @pl.when(inner)
            def _():
                far_copy(what, p, 2 + dx).start()
        y_copy(what, p, 2 * slot + dx).start()
        sib_copy(what, p).start()

    def relay_both(what, slot):
        for dx in range(2):
            relay(what, slot, dx)

    def relay_y(what, slot):
        for dx in range(2):
            p = piece(what, slot, dx, 1)
            wait_piece(what, p)
            sib_copy(what, p).start()

    def wait_sib(what, slot):
        for dy in range(2):
            for dx in range(2):
                p = piece(what, slot, dx, dy)
                reg = region(what, 1 - c, p)
                remote(reg, reg, sib_s.at[what, p], sib_r.at[what, p], sibling).wait_recv()

    greeted = [
        (sibling, None), (at(x, 1 - y, z, c), None), (at(x, y, far, c), None),
        (at(1 - x, y, z, 0), None), (at(1 - x, y, z, 1), None),
        ({"sp": lax.rem(sp + 1, n_sp), "tp": c}, sp < n_sp - 1),
        ({"sp": lax.rem(sp + n_sp - 1, n_sp), "tp": c}, sp > 0),
    ]
    for dz, ok in ((1, z < 3), (-1, z > 0)):
        greeted += [(at(x_, y, z + dz, c_), ok) for x_ in (x, 1 - x) for c_ in range(2)]
    barrier = pltpu.get_barrier_semaphore()
    for dev, ok in greeted:
        def greet():
            pl.semaphore_signal(barrier, inc=1, device_id=dev, device_id_type=MESH)

        if ok is None:
            greet()
        else:
            pl.when(ok)(greet)
    pl.semaphore_wait(barrier, sum(1 if ok is None else ok.astype(jnp.int32) * 1 for _, ok in greeted))

    own_rows = pl.ds(pl.multiple_of(c * half, half), half)
    sib_rows = pl.ds(pl.multiple_of((1 - c) * half, half), half)
    loads = [
        pltpu.make_async_copy(q_hbm, qbuf, load_sem.at[0]),
        pltpu.make_async_copy(k_hbm, kbuf.at[pl.ds(WINDOW, rows)], load_sem.at[1]),
        pltpu.make_async_copy(v_hbm, vbuf.at[pl.ds(WINDOW, rows)], load_sem.at[2]),
        pltpu.make_async_copy(docs_hbm, dbuf.at[pl.ds(1, blocks)], load_sem.at[3]),
        pltpu.make_async_copy(ow_hbm, ow, load_sem.at[4]),
        pltpu.make_async_copy(res_hbm.at[own_rows], res, load_sem.at[5]),
    ]
    for load in loads:
        load.start()

    tail = pl.ds(rows - WINDOW, WINDOW)
    head = pl.ds(0, WINDOW)
    after = {"sp": lax.rem(sp + 1, n_sp), "tp": c}

    halo = [
        remote(k_hbm.at[tail], kbuf.at[head], halo_s.at[0], halo_r.at[0], after),
        remote(v_hbm.at[tail], vbuf.at[head], halo_s.at[1], halo_r.at[1], after),
        remote(docs_hbm.at[blocks - 1], dbuf.at[0], halo_s.at[2], halo_r.at[2], after),
    ]

    @pl.when(sp < n_sp - 1)
    def _():
        for copy in halo:
            copy.start()

    first_sends(GATE_UP, "start", "own")
    first_sends(GATE_UP, "start", "away")

    @pl.when(outer)
    def _():
        first_sends(GATE_UP, "start", "toward")
        first_sends(GATE_UP, "start", "toward_crossing")

    relay(GATE_UP, 0, 0)

    @pl.when(sp == 0)
    def _():
        kbuf[head, :] = jnp.zeros((WINDOW, kbuf.shape[1]), kbuf.dtype)
        vbuf[head, :] = jnp.zeros((WINDOW, vbuf.shape[1]), vbuf.dtype)
        dbuf[0] = jnp.full((1, WINDOW), -1, jnp.int32)

    for load in loads[:4]:
        load.wait()

    def attend_block(n):
        at_rows = pl.ds(pl.multiple_of(n * WINDOW, WINDOW), WINDOW)
        band = pl.ds(pl.multiple_of(n * WINDOW, WINDOW), 2 * WINDOW)
        before_docs, here_docs = dbuf[n], dbuf[n + 1]
        query_docs = jnp.transpose(jnp.broadcast_to(here_docs, (WINDOW, WINDOW)))
        row = lax.broadcasted_iota(jnp.int32, (WINDOW, WINDOW), 0)
        col = lax.broadcasted_iota(jnp.int32, (WINDOW, WINDOW), 1)
        left = (col > row) & (query_docs == before_docs)
        right = (col <= row) & (query_docs == here_docs)
        allowed = jnp.concatenate([left.astype(jnp.int32), right.astype(jnp.int32)], axis=1)
        allowed = jnp.concatenate([allowed] * per_kv, axis=0) != 0
        for j in range(kv_local):
            keys = kbuf[band, j * HD : (j + 1) * HD]
            vals = vbuf[band, j * HD : (j + 1) * HD]
            wide = qbuf[at_rows, j * per_kv * HD : (j + 1) * per_kv * HD]
            query = jnp.concatenate([wide[:, h * HD : (h + 1) * HD] for h in range(per_kv)], axis=0)
            scores = lax.dot_general(
                query, keys, (((1,), (1,)), ((), ())), preferred_element_type=jnp.float32
            ) * HD ** (-0.5)
            scores = jnp.where(allowed, scores, -1e30)
            sink = jnp.concatenate(
                [jnp.full((WINDOW, 1), sink_ref[j * per_kv + h], jnp.float32) for h in range(per_kv)],
                axis=0,
            )
            peak = jnp.maximum(jnp.max(scores, axis=-1, keepdims=True), sink)
            raised = jnp.exp(scores - peak)
            denom = jnp.sum(raised, axis=-1, keepdims=True) + jnp.exp(sink - peak)
            weights = (raised * (1.0 / denom)).astype(jnp.bfloat16)
            mixed = jnp.dot(weights, vals, preferred_element_type=jnp.float32)
            mixed = jnp.concatenate(
                [mixed[h * WINDOW : (h + 1) * WINDOW] for h in range(per_kv)], axis=1
            )
            att[at_rows, j * per_kv * HD : (j + 1) * per_kv * HD] = mixed.astype(jnp.bfloat16)

    def attend_loop(n, carry):
        attend_block(n)
        return carry

    lax.fori_loop(1, blocks, attend_loop, 0)
    relay(GATE_UP, 0, 1)

    @pl.when(inner)
    def _():
        first_sends(GATE_UP, "start", "toward_crossing")
        first_sends(GATE_UP, "start", "toward")

    first_sends(DOWN, "start", "own")

    @pl.when(sp > 0)
    def _():
        for copy in halo:
            copy.wait_recv()

    lax.fori_loop(0, 1, attend_loop, 0)
    loads[4].wait()

    def project(at_rows, dst):
        def body(i, carry):
            cols = pl.ds(pl.multiple_of(i * 256, 256), 256)
            dst[:, cols] = jnp.dot(
                att[at_rows, :], ow[:, cols], preferred_element_type=jnp.float32
            ).astype(jnp.bfloat16)
            return carry

        lax.fori_loop(0, width // 256, body, 0)

    project(sib_rows, mix_out)
    mix_copy = remote(mix_out, mix_in, mix_s, mix_r, sibling)
    mix_copy.start()
    project(own_rows, mix_own)
    loads[5].wait()
    mix_copy.wait_recv()

    base = half

    def norm_body(i, carry):
        at_rows = pl.ds(pl.multiple_of(i * 32, 32), 32)
        mixed = mix_own[at_rows, :].astype(jnp.float32) + mix_in[at_rows, :].astype(jnp.float32)
        stream = (res[at_rows, :].astype(jnp.float32) + mixed).astype(jnp.bfloat16)
        res[at_rows, :] = stream
        floats = stream.astype(jnp.float32)
        scale = lax.rsqrt(jnp.mean(floats * floats, axis=-1, keepdims=True) + 1e-06)
        xbuf[pl.ds(pl.multiple_of(base + i * 32, 32), 32), :] = (
            floats * scale * gain_ref[...]
        ).astype(jnp.bfloat16)
        return carry

    chunk = half // 2

    def rows_of(block, i):
        return xbuf.at[pl.ds(block * half + i * chunk, chunk)]

    def token_copy(kind, i):
        src, dst, dev = {
            0: (3, 2, x_peer),
            1: (1, 0, x_peer),
            2: (1, 3, z_peer),
            3: (0, 2, z_peer),
        }[kind]
        return remote(
            rows_of(src, i), rows_of(dst, i), tok_s.at[kind, i], tok_r.at[kind, i], dev
        )

    pair = 2 * half

    def gate_up(which, slot):
        at_rows = pl.ds(which * pair, pair)
        depths = pl.ds(pl.multiple_of(planes[slot] * slab, slab), slab)

        def body(i, carry):
            cols = pl.ds(pl.multiple_of(i * 256, 256), 256)
            part = jnp.dot(
                xbuf[at_rows, depths], wgu[depths, cols], preferred_element_type=jnp.float32
            )
            acts[at_rows, cols] = part if slot == 0 else acts[at_rows, cols] + part
            return carry

        lax.fori_loop(0, 2 * units // 256, body, 0)

    def gate_up_whole(which, low, high):
        at_rows = pl.ds(which * pair, pair)

        def body(i, carry):
            cols = pl.ds(pl.multiple_of(i * 256, 256), 256)
            acts[at_rows, cols] = jnp.dot(
                xbuf[at_rows, :], wgu[:, cols], preferred_element_type=jnp.float32
            )
            return carry

        lax.fori_loop(low, high, body, 0)

    def activate(which):
        def body(i, carry):
            at_rows = pl.ds(pl.multiple_of(which * pair + i * 32, 32), 32)
            gate, up = acts[at_rows, :units], acts[at_rows, units:]
            hid[at_rows, :] = (gate / (1.0 + jnp.exp(-gate)) * up).astype(jnp.bfloat16)
            return carry

        lax.fori_loop(0, pair // 32, body, 0)

    def slab_cols(slot):
        return pl.ds(pl.multiple_of(down_planes[slot] * slab, slab), slab)

    def x_copy(part, slot):
        i, cols = down_planes[slot], slab_cols(slot)
        dev = z_peer if (part, slot) == (0, 3) else x_peer
        return remote(
            pbuf.at[part, :, cols], rx.at[part, :, cols], rx_s.at[part, i], rx_r.at[part, i], dev
        )

    def z_copy(slot):
        i, cols = down_planes[slot], slab_cols(slot)
        return remote(zbuf.at[:, cols], rz.at[:, cols], rz_s.at[i], rz_r.at[i], z_peer)

    def out_copy(slot):
        part, i = obuf.at[:, slab_cols(slot)], down_planes[slot]
        dst = o_hbm.at[own_rows, slab_cols(slot)]
        return (
            pltpu.make_async_copy(part, dst, out_l.at[i]),
            remote(part, dst, out_s.at[i], out_r.at[i], sibling),
        )

    def over_columns(slot, step):
        def body(i, carry):
            step(pl.ds(pl.multiple_of(down_planes[slot] * slab + i * 256, 256), 256))
            return carry

        lax.fori_loop(0, slab // 256, body, 0)

    def down_first(slot):
        def step(cols):
            part = jnp.dot(hid[:pair, :], wd[:, cols], preferred_element_type=jnp.float32)
            pbuf[1, :, cols] = part[:half].astype(jnp.bfloat16)
            own[:, cols] = part[half:]

        over_columns(slot, step)
        if slot < 3:
            x_copy(1, slot).start()

    def down_second(slot):
        def step(cols):
            part = jnp.dot(hid[pair:, :], wd[:, cols], preferred_element_type=jnp.float32)
            pbuf[0, :, cols] = part[:half].astype(jnp.bfloat16)
            zbuf[:, cols] = part[half:].astype(jnp.bfloat16)

        over_columns(slot, step)
        x_copy(0, slot).start()
        if slot == 3:
            z_copy(slot).start()

    def combine(slot):
        x_copy(0, slot).wait_recv()

        def step(cols):
            mine = zbuf if slot < 3 else pbuf.at[1]
            mine[:, cols] = (
                mine[:, cols].astype(jnp.float32) + rx[0, :, cols].astype(jnp.float32)
            ).astype(jnp.bfloat16)

        over_columns(slot, step)
        (z_copy(slot) if slot < 3 else x_copy(1, slot)).start()

    def finish(slot):
        x_copy(1, slot).wait_recv()
        z_copy(slot).wait_recv()

        def step(cols):
            total = own[:, cols] + rx[1, :, cols].astype(jnp.float32) + rz[:, cols].astype(jnp.float32)
            obuf[:, cols] = (res[:, cols].astype(jnp.float32) + total).astype(jnp.bfloat16)

        over_columns(slot, step)
        for copy in out_copy(slot):
            copy.start()

    def forward_tokens(i, kind):
        token_copy(1 if kind == 3 else 2, i).wait_recv()
        token_copy(kind, i).start()

    def await_tokens(kind):
        for i in range(2):
            token_copy(kind, i).wait_recv()

    def await_diagonal():
        @pl.when(outer)
        def _():
            await_tokens(0)

        @pl.when(inner)
        def _():
            token_copy(2, 0).wait_recv()
            token_copy(3, 0).wait_recv()
            token_copy(0, 1).wait_recv()

    def send_tokens(kind, i):
        token_copy(kind, i).start()

    for i in range(2):
        lax.fori_loop(i * (chunk // 32), (i + 1) * (chunk // 32), norm_body, 0)
        token_copy(1, i).start()

    @pl.when(outer)
    def _():
        send_tokens(2, 0)
        send_tokens(2, 1)

    relay(DOWN, 0, 0, onward=False)

    @pl.when(outer)
    def _():
        relay(DOWN, 0, 1, onward=False)
        relay_both(GATE_UP, 2)

    relay_y(GATE_UP, 0)
    relay_both(GATE_UP, 1)

    @pl.when(inner)
    def _():
        send_tokens(2, 0)
        relay_both(GATE_UP, 2)
        relay_y(GATE_UP, 1)
        relay(GATE_UP, 3, 1)
        send_tokens(2, 1)
        relay(DOWN, 0, 1, onward=False)
        await_tokens(1)
        forward_tokens(1, 0)

    @pl.when(outer)
    def _():
        relay_y(GATE_UP, 2)
        for plane in ("toward_crossing", "toward"):
            first_sends(DOWN, "start", plane)
        forward_tokens(0, 3)
        token_copy(1, 1).wait_recv()
        forward_tokens(0, 0)
        relay_y(GATE_UP, 1)
        relay(GATE_UP, 3, 0)
        relay(GATE_UP, 3, 1)

    wait_sib(GATE_UP, 0)
    gate_up(0, 0)

    @pl.when(inner)
    def _():
        relay(GATE_UP, 3, 0)
        relay_y(GATE_UP, 2)
        for plane in ("away", "toward_crossing", "toward"):
            first_sends(DOWN, "start", plane)

    @pl.when(outer)
    def _():
        forward_tokens(1, 0)

    wait_sib(GATE_UP, 1)
    gate_up(0, 1)
    for dx in range(2):
        far_copy(DOWN, piece(DOWN, 0, dx), dx).start()
    wait_sib(GATE_UP, 2)
    gate_up(0, 2)

    @pl.when(inner)
    def _():
        relay_both(DOWN, 1)

    relay_y(GATE_UP, 3)
    relay_y(DOWN, 0)
    wait_sib(GATE_UP, 3)
    gate_up(0, 3)

    @pl.when(outer)
    def _():
        relay_both(DOWN, 1)

    activate(0)
    wait_sib(DOWN, 0)
    down_first(0)

    @pl.when(inner)
    def _():
        relay_y(DOWN, 1)

    await_diagonal()
    gate_up_whole(1, 0, 4)

    @pl.when(inner)
    def _():
        wait_sib(DOWN, 1)
        down_first(1)

    gate_up_whole(1, 4, 8)
    relay_both(DOWN, 2)
    gate_up_whole(1, 8, 2 * units // 256)
    activate(1)
    down_second(0)
    relay_both(DOWN, 3)

    @pl.when(outer)
    def _():
        relay_y(DOWN, 1)
        wait_sib(DOWN, 1)

    down_second(1)
    relay_y(DOWN, 2)
    combine(0)
    wait_sib(DOWN, 2)
    down_second(2)

    @pl.when(outer)
    def _():
        down_first(1)

    down_first(2)
    combine(1)
    relay_y(DOWN, 3)
    wait_sib(DOWN, 3)
    down_second(3)
    down_first(3)
    combine(2)
    combine(3)
    for slot in range(4):
        finish(slot)

    for slot in range(4):
        for copy in out_copy(slot):
            copy.wait()
        x_copy(0, slot).wait_send()
        x_copy(1, slot).wait_send()
        z_copy(slot).wait_send()

    @pl.when(sp < n_sp - 1)
    def _():
        for copy in halo:
            copy.wait_send()

    mix_copy.wait_send()
    for i in range(2):
        token_copy(1, i).wait_send()
        token_copy(2, i).wait_send()
    token_copy(0, 1).wait_send()

    @pl.when(outer)
    def _():
        token_copy(0, 0).wait_send()
        token_copy(3, 0).wait_send()

    for what in (GATE_UP, DOWN):
        first_sends(what, "wait_send", "own")
        for plane in ("away", "toward", "toward_crossing"):
            first_sends(what, "wait_send", plane)
        for slot in range(4):
            for dx in range(2):
                p = piece(what, slot, dx)
                y_copy(what, p, 2 * slot + dx).wait_send()
                for dy in range(2):
                    sib_copy(what, piece(what, slot, dx, dy)).wait_send()
        for dx in range(2):
            far_copy(what, piece(what, 0, dx), dx).wait_send()

            @pl.when(inner)
            def _():
                far_copy(what, piece(what, 1, dx), 2 + dx).wait_send()


def fused_on_device(
    queries, key_rows, values, doc_ids, sink_logits, residual, out_weight, norm_gain, w_gate, w_up, w_down
):
    rows, width = residual.shape
    half = rows // 2
    units = w_gate.shape[1] // 2
    pieces = lax.axis_size("sp")
    bf16, f32 = jnp.bfloat16, jnp.float32
    anywhere = pl.BlockSpec(memory_space=pl.ANY)
    dma = pltpu.SemaphoreType.DMA
    docs = doc_ids.reshape(rows // WINDOW, 1, WINDOW)
    return pl.pallas_call(
        layer_kernel,
        out_shape=jax.ShapeDtypeStruct((rows, width), bf16),
        in_specs=[
            anywhere, anywhere, anywhere, anywhere,
            pl.BlockSpec(memory_space=pltpu.SMEM),
            anywhere, anywhere,
            pl.BlockSpec(memory_space=pltpu.VMEM),
            anywhere, anywhere, anywhere,
        ],
        out_specs=anywhere,
        scratch_shapes=[
            pltpu.VMEM((width, 2 * units), bf16),
            pltpu.VMEM((units, width), bf16),
            pltpu.VMEM((4 * half, width), bf16),
            pltpu.VMEM((4 * half, 2 * units), f32),
            pltpu.VMEM((4 * half, units), bf16),
            pltpu.VMEM((2, half, width), bf16),
            pltpu.VMEM((half, width), bf16),
            pltpu.VMEM((2, half, width), bf16),
            pltpu.VMEM((half, width), bf16),
            pltpu.VMEM((half, width), f32),
            pltpu.VMEM(queries.shape, bf16),
            pltpu.VMEM((rows + WINDOW, key_rows.shape[1]), bf16),
            pltpu.VMEM((rows + WINDOW, key_rows.shape[1]), bf16),
            pltpu.VMEM((rows // WINDOW + 1, 1, WINDOW), jnp.int32),
            pltpu.VMEM(queries.shape, bf16),
            pltpu.VMEM(out_weight.shape, bf16),
            pltpu.VMEM((half, width), bf16),
            pltpu.VMEM((half, width), bf16),
            pltpu.VMEM((half, width), bf16),
            pltpu.VMEM((half, width), bf16),
            pltpu.VMEM((half, width), bf16),
            dma((6,)), dma((3,)), dma((3,)), dma((2, 2, 4)), dma((2,)), dma((2, 4)), dma((2, 8)),
            dma((2, pieces)), dma((2, pieces)), dma((2, pieces)),
            dma, dma, dma((4, 2)), dma((4, 2)), dma((2, 4)), dma((2, 4)), dma((4,)), dma((4,)),
            dma((4,)), dma((4,)), dma((4,)),
        ],
        compiler_params=pltpu.CompilerParams(has_side_effects=True, collective_id=0, vmem_limit_bytes=63 * 2**20),
        name="layer",
    )(
        queries, key_rows, values, docs, sink_logits, residual, out_weight,
        norm_gain.reshape(1, width), w_gate, w_up, w_down,
    )


def solution(mesh):
    if (mesh.shape["sp"], mesh.shape["tp"]) != (16, 2):
        return staged_solution(mesh)
    in_specs = (
        P("sp", "tp"), P("sp", "tp"), P("sp", "tp"), P("sp"), P("tp"), P("sp", None), P("tp", None),
        P(), P("sp", "tp"), P("sp", "tp"), P("tp", "sp"),
    )
    return jax.shard_map(
        fused_on_device, mesh=mesh, in_specs=in_specs, out_specs=P("sp", None), check_vma=False
    )
```
